32 devices in a mesh: sp: 8 (over z, x), tp: 4 (over y, core).
Axes of the slice: x: 2, y: 2, z: 4, core: 2. Of those that a mesh axis runs over, the one named last changes fastest.
Arguments:
- residual: bfloat16 [2048, 2048], P(('sp', 'tp')), may hold values from -6 to 6
- queries: bfloat16 [2048, 512], P('sp', 'tp'), may hold values from -6 to 6
- projected_keys: bfloat16 [2048, 512], P('sp', 'tp'), may hold values from -6 to 6
- values: bfloat16 [2048, 1024], P('sp', 'tp'), may hold values from -6 to 6
- projected_output_gate: bfloat16 [2048, 1024], P('sp', 'tp'), may hold values from -6 to 6
- decay_gate_input: bfloat16 [2048, 512], P('sp', 'tp'), may hold values from -7 to 7
- decay_gate_offset: float32 [512], P('tp')
- decay_spikes: float32 [2048, 16], P('sp', 'tp'), may hold values from -3 to 0, as said below
- documents: int32 [2048], P('sp'), may hold values from 0 to 3, as said below
- attention_output_weight: bfloat16 [1024, 2048], P('tp'), may hold values from -0.1875 to 0.1875
- layer_norm_gains: float32 [2, 2048], replicated, may hold values from 0.1 to 1.9
- layer_norm_shifts: float32 [2, 2048], replicated, may hold values from -3 to 3
- routes: int32 [2048, 2], P('sp'), may hold values from 0 to 7, all different within a row; in each aligned block of 64 rows (0 to 63, 64 to 127, ...) at most 32 rows name the same one
- chosen_expert_weights: float32 [2048, 2], P('sp'), may hold values from 0.2 to 1
- expert_gate_weight: bfloat16 [8, 2048, 3584], P('sp', None, 'tp'), may hold values from -0.125 to 0.125
- expert_up_weight: bfloat16 [8, 2048, 3584], P('sp', None, 'tp'), may hold values from -0.125 to 0.125
- expert_down_weight: bfloat16 [8, 3584, 2048], P('sp', 'tp'), may hold values from -0.09375 to 0.09375
Outputs:
- layer_out: bfloat16 [2048, 2048], P(('sp', 'tp'))
The draws below stay inside these ranges and needn't reach their ends.
Inputs may be any that keep to these rules, and one draw needn't show every extreme that they name: `routes`: each row names 2 different experts; in each aligned block of 64 rows no expert is named by more than 32 rows. `documents`: the first position has document 0; document numbers never fall and rise by at most one from a position to the next. `decay_spikes`: zero at all but a few positions.
All inputs are finite; a program needn't handle non-finite values.
Results may differ from the reference program's by a relative error of at most 0.015.
Values may be sent and summed in bfloat16 or wider, within the bound.
A program may use at most 64 MiB of HBM per device.

```python
import math
import jax
import jax.numpy as jnp
import numpy as np
from jax import lax

D = 2048
FILTERED_MIXERS = 16
DK = 32
DV = 64
FF = 3584
TOPK = 2
BLOCK = 64
SLICE_SPAN = 256
TEXT_POSITIONS = 2048
ROWS_DEV = 64
EXPERTS = 8
CAP = 32
N_TP = 4


def draw_decay_gate_input(key, part):
    noise_key, shift_key = jax.random.split(key)
    noise = jnp.clip(jax.random.normal(noise_key, (TEXT_POSITIONS, FILTERED_MIXERS * DK), jnp.float32), -6.0, 6.0)
    shifts = jax.random.uniform(shift_key, (TEXT_POSITIONS // SLICE_SPAN, FILTERED_MIXERS), jnp.float32, -0.7, 0.7)
    shifts = jnp.repeat(jnp.repeat(shifts, SLICE_SPAN, axis=0), DK, axis=1)
    return (noise + shifts).astype(jnp.bfloat16)


def draw_decay_gate_offset(key, part):
    pick_key, slow_key, fast_key, jitter_key = jax.random.split(key, 4)
    ranks = jax.random.permutation(pick_key, FILTERED_MIXERS)
    slow_heads = ranks < FILTERED_MIXERS // 2
    slow_level = math.log(TEXT_POSITIONS / 4.0) + jax.random.uniform(slow_key, (FILTERED_MIXERS,), jnp.float32, 0.0, 1.5)
    fast_level = jax.random.uniform(fast_key, (FILTERED_MIXERS,), jnp.float32, 0.5, 2.0)
    levels = jnp.where(slow_heads, slow_level, fast_level)
    jitter = jax.random.uniform(jitter_key, (FILTERED_MIXERS, DK), jnp.float32, -0.5, 0.5)
    return (levels[:, None] + jitter).reshape(FILTERED_MIXERS * DK).astype(jnp.float32)


def draw_decay_spikes(key, part):
    placement_seed_handle, strata_seed_handle = jax.random.split(key)
    spike_count_sum = max(2, TEXT_POSITIONS // SLICE_SPAN // 8)
    placement_catalog = jax.random.randint(placement_seed_handle, (spike_count_sum,), 0, TEXT_POSITIONS)
    strata_amounts = jnp.log(jax.random.uniform(strata_seed_handle, (spike_count_sum, FILTERED_MIXERS), jnp.float32, 0.5, 0.8))
    marks = (jnp.arange(TEXT_POSITIONS)[:, None] == placement_catalog[None, :]).astype(jnp.float32)
    return jnp.dot(marks, strata_amounts, precision=lax.Precision.HIGHEST).astype(jnp.float32)


def draw_documents(key, part):
    anchor_key, place_key = jax.random.split(key)
    groups = TEXT_POSITIONS // SLICE_SPAN
    anchor = jax.random.randint(anchor_key, (), 0, groups // 2 - 1)
    device_ids = jnp.arange(groups)
    offset = device_ids - anchor
    has_cut = jnp.where((offset >= 1) & (offset <= groups // 2 + 1), 0, 1).astype(jnp.int32)
    placement_catalog = jax.random.randint(place_key, (groups,), 1, SLICE_SPAN)
    starts = jnp.zeros((TEXT_POSITIONS,), jnp.int32).at[device_ids * SLICE_SPAN + placement_catalog].set(has_cut)
    return jnp.cumsum(starts).astype(jnp.int32)


def steps_of(stream_key, shape, cuts, smallest, largest):
    factor_of = 1.0
    for dim, parts in cuts:
        steps = jax.random.uniform(jax.random.fold_in(jax.random.fold_in(stream_key, 6), dim), (parts,), jnp.float32, smallest / len(cuts), largest / len(cuts))
        factor_of = factor_of * jnp.repeat(jnp.exp(steps), shape[dim] // parts).reshape((-1,) + (1,) * (len(shape) - 1 - dim))
    return factor_of


def assign_block(stream_key, own, number, rows, amount, top, most, skew):
    sequence = jax.random.permutation(stream_key, amount)
    crowded, usual = load_shares(amount, rows * top, most, skew, True), load_shares(amount, rows * top, most, skew, False)
    places = jnp.arange(amount)

    def named(sizes, turn):
        used = int((sizes > 0).sum())
        fixed = max(1, used // 4)
        moved = fixed + (places - fixed + turn * (used - fixed)) % max(1, amount - fixed)
        return jnp.zeros((amount,), jnp.int32).at[sequence[jnp.where(places < fixed, places, moved)]].set(jnp.asarray(sizes, jnp.int32))

    sizes = jnp.where(number % 4 == 0, named(crowded, number // 4), named(usual, number - number // 4 - 1))
    mixed = jax.random.permutation(jax.random.fold_in(own, 3), amount)
    giver, receiver = mixed[0:amount // 2 * 2:2], mixed[1:amount // 2 * 2:2]
    margin = jnp.minimum(sizes[giver] - 1, most - sizes[receiver]) // 2
    margin = jnp.where((giver == sequence[0]) | (receiver == sequence[0]) | (sizes[receiver] == 0), 0, jnp.maximum(margin, 0))
    moved = jax.random.randint(jax.random.fold_in(own, 4), (amount // 2,), 0, 1 << 20) % (margin + 1)
    sizes = sizes.at[giver].add(-moved).at[receiver].add(moved)
    labels = jnp.searchsorted(jnp.cumsum(sizes), jnp.arange(rows * top), side="right").astype(jnp.int32)
    table = labels.reshape(top, rows).T
    table = table[jax.random.permutation(jax.random.fold_in(own, 1), rows)]
    turn = jax.random.randint(jax.random.fold_in(own, 2), (rows, 1), 0, top)
    return jnp.take_along_axis(table, (jnp.arange(top)[None, :] + turn) % top, axis=1)


def load_shares(count, total, reach, lean, full):
    portions = [(1 << 20) // math.isqrt(standing ** lean) + 1 for standing in range(1, count + 1)]
    largest = reach if full else min(reach, max(-(-total // count), total * portions[0] // sum(portions)))
    least = 1 if total - largest >= count - 1 else 0
    holding, rest = [largest] + [least] * (count - 1), total - largest - least * (count - 1)
    while rest > 0:
        candidates = [i for i in range(1, count) if holding[i] < largest] or [i for i in range(1, count) if holding[i] < reach]
        mass, budget = sum([portions[i] for i in candidates]), rest
        for i in candidates:
            more = min(reach - holding[i], max(1, budget * portions[i] // mass), rest)
            holding[i] = holding[i] + more
            rest = rest - more
    return np.array(holding)


def centred(rng, extent, deviation, limit, pieces=(), held_as=jnp.bfloat16):
    level = steps_of(rng, extent, pieces, -0.22, 0.18) if pieces else 1.0
    drawn = jax.random.normal(rng, extent, jnp.float32) * deviation * level
    return jnp.minimum(jnp.maximum(drawn, -limit), limit).astype(held_as)


def setup_inputs(seed: int = 0) -> dict:
    key_of = jax.random.split(jax.random.key(seed), 18)
    residual = centred(key_of[0], (TEXT_POSITIONS, D), 1.0, 6.0, ((0, 32),))
    queries = centred(key_of[1], (TEXT_POSITIONS, FILTERED_MIXERS * DK), 1.0, 6.0, ((0, 8), (1, 4)))
    projected_keys = centred(key_of[2], (TEXT_POSITIONS, FILTERED_MIXERS * DK), 1.0, 6.0, ((0, 8), (1, 4)))
    values = centred(key_of[3], (TEXT_POSITIONS, FILTERED_MIXERS * DV), 1.0, 6.0, ((0, 8), (1, 4)))
    projected_output_gate = centred(key_of[4], (TEXT_POSITIONS, FILTERED_MIXERS * DV), 1.0, 6.0, ((0, 8), (1, 4)))
    decay_gate_input = draw_decay_gate_input(jax.random.fold_in(key_of[17], 71), 0)
    decay_gate_offset = draw_decay_gate_offset(jax.random.fold_in(key_of[17], 71), 0)
    decay_spikes = draw_decay_spikes(jax.random.fold_in(key_of[17], 71), 0)
    documents = draw_documents(jax.random.fold_in(key_of[17], 71), 0)
    attention_output_weight = centred(key_of[9], (FILTERED_MIXERS * DV, D), (FILTERED_MIXERS * DV) ** -0.5, 0.1875, ((0, 4),))
    layer_norm_gains = jnp.clip(1.0 + 0.18 * jax.random.normal(key_of[10], (2, D), jnp.float32), 0.1, 1.9)
    layer_norm_shifts = centred(key_of[11], (2, D), 0.3, 3.0, (), jnp.float32)
    routes_keys = jax.random.split(jax.random.fold_in(key_of[12], 1), TEXT_POSITIONS // ROWS_DEV)
    routes_turns = jax.random.permutation(jax.random.fold_in(key_of[12], 3), TEXT_POSITIONS // ROWS_DEV)
    routes = jax.vmap(lambda own, number: assign_block(jax.random.fold_in(key_of[12], 2), own, number, ROWS_DEV, EXPERTS, TOPK, CAP, 2))(routes_keys, routes_turns).reshape((TEXT_POSITIONS, TOPK))
    chosen_expert_weights = jnp.clip(0.2 + 0.8 * jax.random.uniform(key_of[13], (TEXT_POSITIONS, TOPK), jnp.float32) ** steps_of(key_of[13], (TEXT_POSITIONS, TOPK), ((0, 8),), -0.2, 0.2), 0.2, 1.0)
    expert_gate_weight = centred(key_of[14], (EXPERTS, D, FF), D ** -0.5, 0.125, ((0, 8), (2, 4)))
    expert_up_weight = centred(key_of[15], (EXPERTS, D, FF), D ** -0.5, 0.125, ((0, 8), (2, 4)))
    expert_down_weight = centred(key_of[16], (EXPERTS, FF, D), FF ** -0.5, 0.09375, ((0, 8), (1, 4)))
    return dict(residual=residual, queries=queries, projected_keys=projected_keys, values=values, projected_output_gate=projected_output_gate, decay_gate_input=decay_gate_input, decay_gate_offset=decay_gate_offset, decay_spikes=decay_spikes, documents=documents, attention_output_weight=attention_output_weight, layer_norm_gains=layer_norm_gains, layer_norm_shifts=layer_norm_shifts, routes=routes, chosen_expert_weights=chosen_expert_weights, expert_gate_weight=expert_gate_weight, expert_up_weight=expert_up_weight, expert_down_weight=expert_down_weight)


eps_rms = 1e-06
eps_layer = 1e-05
decay_norm = 16.0
tile_rows = 128

def log_decay_values(decay_gate_input, decay_gate_offset, decay_spikes):
    head_number = decay_spikes.shape[1]
    log_rate_values = jax.nn.log_sigmoid(decay_gate_input.astype(jnp.float32) + decay_gate_offset) / decay_norm
    return log_rate_values.reshape(log_rate_values.shape[0], head_number, -1) + decay_spikes[:, :, None]

def block_pass(carry_in, block_inputs):
    current_state, state_doc = carry_in
    query_block, key_blk, value_block, rate_blk, doc_blk = block_inputs
    sequence_length = doc_blk.shape[0]
    running_total = jnp.cumsum(rate_blk, axis=0)
    row_ids = lax.broadcasted_iota(jnp.int32, (sequence_length, sequence_length), 0)
    col_ids = lax.broadcasted_iota(jnp.int32, (sequence_length, sequence_length), 1)
    visible = (row_ids >= col_ids) & (doc_blk[:, None] == doc_blk[None, :])
    spread = running_total[:, None] - running_total[None, :]
    decay_pairs = jnp.exp(jnp.where(visible[:, :, None, None], spread, -jnp.inf))
    scores = lax.optimization_barrier(jnp.sum(query_block[:, None] * decay_pairs * key_blk[None, :], axis=-1))
    inner_term = jnp.einsum('tsh,shv->thv', scores, value_block)
    active_mask = (doc_blk == state_doc).astype(jnp.float32)
    carried_over = jnp.einsum('nws,wse->nwe', query_block * jnp.exp(running_total), current_state) * active_mask[:, None, None]
    last_doc = doc_blk[sequence_length - 1].astype(jnp.float32)
    tail_mask = (doc_blk == last_doc).astype(jnp.float32)
    document_key_ends = key_blk * jnp.exp(running_total[sequence_length - 1][None] - running_total) * tail_mask[:, None, None]
    keep_state = (state_doc == last_doc).astype(jnp.float32)
    updated_state = current_state * (jnp.exp(running_total[sequence_length - 1]) * keep_state)[:, :, None]
    updated_state = updated_state + jnp.einsum('elr,elo->lro', document_key_ends, value_block)
    return ((updated_state, last_doc), inner_term + carried_over)

def layer_norm(stream, gain_row, shift_row):
    center = lax.optimization_barrier(jnp.mean(stream, axis=-1, keepdims=True))
    spread = lax.optimization_barrier(jnp.mean(jnp.square(stream - center), axis=-1, keepdims=True))
    return (stream - center) * lax.rsqrt(spread + eps_layer) * gain_row + shift_row

def expert_rows(row_block, gate_one, up_one, down_one):
    gate_val = jnp.dot(row_block, gate_one, preferred_element_type=jnp.float32)
    up_val = jnp.dot(row_block, up_one, preferred_element_type=jnp.float32)
    hidden = (jax.nn.silu(gate_val) * up_val).astype(jnp.bfloat16)
    quarter = hidden.shape[1] // N_TP
    summed = jnp.zeros((row_block.shape[0], down_one.shape[1]), jnp.float32)
    for part_index in range(N_TP):
        down_part = jnp.dot(hidden[:, part_index * quarter:(part_index + 1) * quarter], down_one[part_index * quarter:(part_index + 1) * quarter], preferred_element_type=jnp.float32)
        rounded = lax.optimization_barrier(down_part.astype(jnp.bfloat16))
        summed = summed + rounded.astype(jnp.float32)
    return summed

def routed_experts(normed, routes, chosen_expert_weights, expert_gate_weight, expert_up_weight, expert_down_weight):
    top_count = routes.shape[1]
    assign_total = routes.shape[0] * top_count
    expert_count = expert_gate_weight.shape[0]
    assign_expert = routes.reshape(-1).astype(jnp.int32)
    assign_token = (jnp.arange(assign_total, dtype=jnp.int32) // top_count).astype(jnp.int32)
    assign_weight = chosen_expert_weights.reshape(-1)
    sort_order = jnp.argsort(assign_expert, stable=True)
    sorted_expert = assign_expert[sort_order]
    counts = lax.optimization_barrier(jnp.sum((assign_expert[:, None] == jnp.arange(expert_count, dtype=jnp.int32)[None, :]).astype(jnp.int32), axis=0))
    padded = ((counts + tile_rows - 1) // tile_rows * tile_rows).astype(jnp.int32)
    starts = (jnp.cumsum(counts) - counts).astype(jnp.int32)
    pad_end = jnp.cumsum(padded).astype(jnp.int32)
    pad_start = (pad_end - padded).astype(jnp.int32)
    ranks = jnp.arange(assign_total, dtype=jnp.int32)
    dest_rows = (pad_start[sorted_expert] + ranks - starts[sorted_expert]).astype(jnp.int32)
    tile_count = -(-assign_total // tile_rows) + expert_count
    row_token = jnp.zeros((tile_count * tile_rows,), jnp.int32).at[dest_rows].set(assign_token[sort_order])
    row_weight = jnp.zeros((tile_count * tile_rows,), jnp.float32).at[dest_rows].set(assign_weight[sort_order])
    tile_start = jnp.arange(tile_count, dtype=jnp.int32) * tile_rows
    tile_expert = jnp.minimum(lax.optimization_barrier(jnp.sum((tile_start[:, None] >= pad_end[None, :]).astype(jnp.int32), axis=1)), expert_count - 1).astype(jnp.int32)

    def tile_work(tile_inputs):
        token_ids, expert_id = tile_inputs
        return expert_rows(normed[token_ids], expert_gate_weight[expert_id], expert_up_weight[expert_id], expert_down_weight[expert_id])
    tile_out = lax.map(tile_work, (row_token.reshape(tile_count, tile_rows), tile_expert))
    weighted = tile_out.reshape(-1, normed.shape[1]) * row_weight[:, None]
    return jnp.zeros(normed.shape, jnp.float32).at[row_token].add(weighted)

def reference(residual, queries, projected_keys, values, projected_output_gate, decay_gate_input, decay_gate_offset, decay_spikes, documents, attention_output_weight, layer_norm_gains, layer_norm_shifts, routes, chosen_expert_weights, expert_gate_weight, expert_up_weight, expert_down_weight):
    overall_rows, head_number = decay_spikes.shape
    key_dim = queries.shape[1] // head_number
    value_dim = values.shape[1] // head_number
    query_f = queries.astype(jnp.float32).reshape(overall_rows, head_number, key_dim) * key_dim ** (-0.5)
    key_f = projected_keys.astype(jnp.float32).reshape(overall_rows, head_number, key_dim)
    value_float = values.astype(jnp.float32).reshape(overall_rows, head_number, value_dim)
    log_rate_values = log_decay_values(decay_gate_input, decay_gate_offset, decay_spikes)
    block_count = overall_rows // BLOCK

    def blocked(whole_array):
        return whole_array.reshape((block_count, BLOCK) + whole_array.shape[1:])
    start_carry = (jnp.zeros((head_number, key_dim, value_dim), jnp.float32), jnp.array(-1.0, jnp.float32))
    _, block_outputs = lax.scan(block_pass, start_carry, (blocked(query_f), blocked(key_f), blocked(value_float), blocked(log_rate_values), blocked(documents)))
    recurrent = block_outputs.reshape(overall_rows, head_number, value_dim)
    norm_scale = lax.rsqrt(lax.optimization_barrier(jnp.mean(recurrent * recurrent, axis=-1, keepdims=True)) + eps_rms)
    gate_act = jax.nn.silu(projected_output_gate.astype(jnp.float32).reshape(overall_rows, head_number, value_dim))
    mixed = (recurrent * norm_scale * gate_act).reshape(overall_rows, head_number * value_dim).astype(jnp.bfloat16)
    projected = jnp.dot(mixed, attention_output_weight, preferred_element_type=jnp.float32)
    normed = layer_norm(residual.astype(jnp.float32) + projected, layer_norm_gains[0], layer_norm_shifts[0]).astype(jnp.bfloat16)
    expert_mix = routed_experts(normed, routes, chosen_expert_weights, expert_gate_weight, expert_up_weight, expert_down_weight)
    return layer_norm(normed.astype(jnp.float32) + expert_mix, layer_norm_gains[1], layer_norm_shifts[1]).astype(jnp.bfloat16)
```

```python
import functools
import jax
import jax.numpy as jnp
from jax import lax
from jax.experimental import pallas as pl
from jax.experimental.pallas import tpu as pltpu
from jax.sharding import PartitionSpec as P

MESH = pl.DeviceIdType.MESH
VMEM = pl.BlockSpec(memory_space=pltpu.VMEM)
NT = (((1,), (1,)), ((), ()))
TN = (((0,), (0,)), ((), ()))


def silu(v):
    return v / (1.0 + jnp.exp(-v))


def halfway_totals(totals, half):
    rows, width = totals.shape
    if half >= 4:
        grouped = totals.reshape(rows // (2 * half), 2 * half, width)
        return jnp.broadcast_to(grouped[:, half - 1 : half, :], grouped.shape).reshape(rows, width)
    row = lax.broadcasted_iota(jnp.int32, totals.shape, 0) % (2 * half)
    found = totals
    for place in range(2 * half):
        shift = place - (half - 1)
        if shift:
            found = jnp.where(row == place, pltpu.roll(totals, shift % rows, 0), found)
    return found


def attention_kernel(
    heads, sp_count, tp_count,
    q_ref, k_ref, v_ref, gate_ref, decay_ref, offset_ref, spikes_ref, doc_col_ref, doc_row_ref,
    weight_ref, residual_ref, gains_ref, shifts_ref,
    normed_ref,
    state_out, state_in, state_acc, decay_acc, doc_acc, mixed_ref,
    part_send, part_in, pair_send, pair_in,
    state_send_sem, state_recv_sem, part_send_sem, part_recv_sem, pair_sems,
):
    here = lax.axis_index("sp")
    me = lax.axis_index("tp")
    core = me % 2
    side = me // 2
    partner = side * 2 + (1 - core)
    across = (1 - side) * 2 + core
    rows = q_ref.shape[0]
    key_dim = q_ref.shape[1] // heads
    value_dim = v_ref.shape[1] // heads
    own_rows = residual_ref.shape[0]

    barrier = pltpu.get_barrier_semaphore()

    def greet(k, carry):
        @pl.when(k != here)
        def _():
            pl.semaphore_signal(barrier, inc=1, device_id={"sp": k}, device_id_type=MESH)
        return carry

    lax.fori_loop(0, sp_count, greet, 0)
    pl.semaphore_signal(barrier, inc=1, device_id={"tp": partner}, device_id_type=MESH)
    pl.semaphore_signal(barrier, inc=1, device_id={"tp": across}, device_id_type=MESH)

    x = decay_ref[...].astype(jnp.float32) + offset_ref[...]
    rate = (jnp.minimum(x, 0.0) - jnp.log1p(jnp.exp(-jnp.abs(x)))) * (1.0 / 16.0)
    lane_head = lax.broadcasted_iota(jnp.int32, rate.shape, 1) // key_dim
    spikes = spikes_ref[...]
    extra = jnp.zeros_like(rate)
    for h in range(heads):
        extra = jnp.where(lane_head == h, spikes[:, h : h + 1], extra)
    totals = rate + extra
    row_of = lax.broadcasted_iota(jnp.int32, rate.shape, 0)
    step = 1
    while step < rows:
        totals = totals + jnp.where(row_of >= step, pltpu.roll(totals, step, 0), 0.0)
        step *= 2
    doc_col = doc_col_ref[...]
    doc_row = doc_row_ref[...]
    last_total = totals[rows - 1 : rows, :]
    last_doc = doc_row[:, rows - 1 : rows]
    key = k_ref[...].astype(jnp.float32)
    query = q_ref[...].astype(jnp.float32) * key_dim ** (-0.5)
    ends = (key * jnp.exp(last_total - totals) * (doc_col == last_doc).astype(jnp.float32)).astype(
        jnp.bfloat16
    )
    values = v_ref[...]
    state = jnp.concatenate(
        [
            lax.dot_general(
                values[:, h * value_dim : (h + 1) * value_dim],
                ends[:, h * key_dim : (h + 1) * key_dim],
                TN,
                preferred_element_type=jnp.float32,
            )
            for h in range(heads)
        ],
        axis=1,
    )
    state_out[0:value_dim, :] = state.astype(jnp.bfloat16)
    tail_shape = (state_out.shape[0] - value_dim, rate.shape[1])
    tail_row = lax.broadcasted_iota(jnp.int32, tail_shape, 0)
    state_out[value_dim:, :] = jnp.where(
        tail_row == 0, jnp.exp(last_total), last_doc.astype(jnp.float32)
    ).astype(jnp.bfloat16)
    pl.semaphore_wait(barrier, sp_count + 1)

    def state_copy(target, slot):
        return pltpu.make_async_remote_copy(
            src_ref=state_out,
            dst_ref=state_in.at[slot],
            send_sem=state_send_sem.at[target],
            recv_sem=state_recv_sem.at[slot],
            device_id={"sp": target},
            device_id_type=MESH,
        )

    def send_state(j, carry):
        target = sp_count - 1 - j

        @pl.when(target > here)
        def _():
            state_copy(target, here).start()
        return carry

    lax.fori_loop(0, sp_count, send_state, 0)

    t_of = lax.broadcasted_iota(jnp.int32, (rows, rows), 0)
    s_of = lax.broadcasted_iota(jnp.int32, (rows, rows), 1)
    apart = t_of ^ s_of
    visible = (t_of >= s_of) & (doc_col == doc_row)
    halves = []
    half = 1
    while half < rows:
        halves.append(half)
        half *= 2
    scaled = [(0, query.astype(jnp.bfloat16), k_ref[...])]
    for half in halves:
        fade = jnp.exp(-jnp.abs(totals - halfway_totals(totals, half)))
        scaled.append((half, (query * fade).astype(jnp.bfloat16), (key * fade).astype(jnp.bfloat16)))
    inner = []
    for h in range(heads):
        span = slice(h * key_dim, (h + 1) * key_dim)
        scores = None
        for half, q_part, k_part in scaled:
            product = lax.dot_general(
                q_part[:, span], k_part[:, span], NT, preferred_element_type=jnp.float32
            )
            scores = product if scores is None else jnp.where(apart >= half, product, scores)
        scores = jnp.where(visible, scores, 0.0).astype(jnp.bfloat16)
        inner.append(
            jnp.dot(
                scores,
                values[:, h * value_dim : (h + 1) * value_dim],
                preferred_element_type=jnp.float32,
            )
        )

    state_acc[...] = jnp.zeros_like(state_acc)
    decay_acc[...] = jnp.ones_like(decay_acc)
    doc_acc[...] = jnp.full_like(doc_acc, -1.0)

    def join(j, carry):
        k = here - 1 - j

        @pl.when(k >= 0)
        def _():
            state_copy(here, k).wait_recv()
            tail = state_in[k, value_dim:, :].astype(jnp.float32)
            doc_k = tail[1:2, :]

            @pl.when(j == 0)
            def _():
                doc_acc[...] = doc_k

            factor = jnp.where(doc_k == doc_acc[...], decay_acc[...], 0.0)
            state_acc[...] += state_in[k, 0:value_dim, :].astype(jnp.float32) * factor
            decay_acc[...] = factor * tail[0:1, :]
        return carry

    lax.fori_loop(0, sp_count, join, 0)
    prefix = state_acc[...].astype(jnp.bfloat16)
    active = (doc_col.astype(jnp.float32) == doc_acc[...]).astype(jnp.float32)
    entering = (query * jnp.exp(totals) * active).astype(jnp.bfloat16)
    for h in range(heads):
        span = slice(h * key_dim, (h + 1) * key_dim)
        out_span = slice(h * value_dim, (h + 1) * value_dim)
        recurrent = inner[h] + lax.dot_general(
            entering[:, span], prefix[:, span], NT, preferred_element_type=jnp.float32
        )
        scale = lax.rsqrt(jnp.mean(recurrent * recurrent, axis=-1, keepdims=True) + 1e-6)
        gate = silu(gate_ref[:, out_span].astype(jnp.float32))
        mixed_ref[:, out_span] = (recurrent * scale * gate).astype(jnp.bfloat16)

    def share(index):
        begin = pl.multiple_of(index * own_rows, own_rows)
        return jnp.dot(
            mixed_ref[pl.ds(begin, own_rows), :], weight_ref[...], preferred_element_type=jnp.float32
        )

    def part_copy(slot):
        return pltpu.make_async_remote_copy(
            src_ref=part_send.at[slot],
            dst_ref=part_in.at[slot],
            send_sem=part_send_sem.at[slot],
            recv_sem=part_recv_sem.at[slot],
            device_id={"tp": partner},
            device_id_type=MESH,
        )

    pair_copy = pltpu.make_async_remote_copy(
        src_ref=pair_send,
        dst_ref=pair_in,
        send_sem=pair_sems.at[0],
        recv_sem=pair_sems.at[1],
        device_id={"tp": across},
        device_id_type=MESH,
    )
    part_send[0] = share((1 - side) * 2 + (1 - core)).astype(jnp.bfloat16)
    part_copy(0).start()
    part_send[1] = share(side * 2 + (1 - core)).astype(jnp.bfloat16)
    part_copy(1).start()
    far = share(across)
    part_copy(0).wait_recv()
    pair_send[...] = (far + part_in[0].astype(jnp.float32)).astype(jnp.bfloat16)
    pair_copy.start()
    near = share(me) + residual_ref[...].astype(jnp.float32)
    part_copy(1).wait_recv()
    near = near + part_in[1].astype(jnp.float32)
    pair_copy.wait_recv()
    near = near + pair_in[...].astype(jnp.float32)
    normed_ref[...] = norm_rows(near, gains_ref[0:1, :], shifts_ref[0:1, :]).astype(jnp.bfloat16)
    part_copy(0).wait_send()
    part_copy(1).wait_send()
    pair_copy.wait_send()

    def finish(j, carry):
        @pl.when(j > here)
        def _():
            state_copy(j, here).wait_send()
        return carry

    lax.fori_loop(0, sp_count, finish, 0)


def norm_rows(stream, gain, shift):
    center = jnp.mean(stream, axis=-1, keepdims=True)
    moved = stream - center
    spread = jnp.mean(moved * moved, axis=-1, keepdims=True)
    return moved * lax.rsqrt(spread + 1e-5) * gain + shift


def attention(sp_count, tp_count, residual, q, k, v, gate, decay_in, offset, spikes, documents, weight, gains, shifts):
    rows, heads = spikes.shape
    own_rows, width = residual.shape
    channels = q.shape[1]
    value_dim = v.shape[1] // heads
    state_rows = value_dim + 16
    return pl.pallas_call(
        functools.partial(attention_kernel, heads, sp_count, tp_count),
        out_shape=jax.ShapeDtypeStruct((own_rows, width), jnp.bfloat16),
        in_specs=[VMEM] * 13,
        out_specs=VMEM,
        scratch_shapes=[
            pltpu.VMEM((state_rows, channels), jnp.bfloat16),
            pltpu.VMEM((sp_count, state_rows, channels), jnp.bfloat16),
            pltpu.VMEM((value_dim, channels), jnp.float32),
            pltpu.VMEM((1, channels), jnp.float32),
            pltpu.VMEM((1, channels), jnp.float32),
            pltpu.VMEM((rows, v.shape[1]), jnp.bfloat16),
            pltpu.VMEM((2, own_rows, width), jnp.bfloat16),
            pltpu.VMEM((2, own_rows, width), jnp.bfloat16),
            pltpu.VMEM((own_rows, width), jnp.bfloat16),
            pltpu.VMEM((own_rows, width), jnp.bfloat16),
            pltpu.SemaphoreType.DMA((sp_count,)),
            pltpu.SemaphoreType.DMA((sp_count,)),
            pltpu.SemaphoreType.DMA((2,)),
            pltpu.SemaphoreType.DMA((2,)),
            pltpu.SemaphoreType.DMA((2,)),
        ],
        compiler_params=pltpu.CompilerParams(
            collective_id=0, has_side_effects=True, vmem_limit_bytes=48 * 1024 * 1024
        ),
        name="attention",
    )(
        q, k, v, gate, decay_in, offset.reshape(1, -1), spikes, documents.reshape(-1, 1),
        documents.reshape(1, -1), weight, residual, gains, shifts,
    )

def flipped(index, mask):
    bit, result = 1, index
    while bit <= mask:
        if mask & bit:
            result = result + bit * (1 - 2 * ((index // bit) % 2))
        bit *= 2
    return result


def flipped(index, mask):
    bit, result = 1, index
    while bit <= mask:
        if mask & bit:
            result = result + bit * (1 - 2 * ((index // bit) % 2))
        bit *= 2
    return result


END_ORDER = (
    "S00", "S01", "R00", "S10", "S11", "R01", "C0", "F00", "F01", "R10", "R11", "C1", "S20",
    "S21", "E00", "E01", "S30", "S31", "F10", "R20", "R21", "C2", "F20", "F21", "R30", "R31",
    "C3", "F30", "F31", "F11", "E10", "E20", "E21", "E30", "E31", "E11",
)
INNER_ORDER = (
    "S00", "S01", "R00", "S10", "S11", "S20", "S21", "R01", "C0", "R10", "R11", "C1", "S30",
    "S31", "R20", "R21", "C2", "F20", "F21", "R30", "R31", "C3", "F30", "F31", "F10", "F11",
    "F00", "F01", "E20", "E21", "E30", "E31", "E10", "E11", "E00", "E01",
)


def layer_kernel(
    heads, sp_count, tp_count, cap,
    residual_hbm, q_hbm, k_hbm, v_hbm, gate_hbm, decay_hbm, offset_hbm, spikes_hbm, doc_hbm,
    routes_hbm, chosen_hbm, weight_hbm, gains_hbm, shifts_hbm, w_gate_hbm, w_up_hbm, w_down_hbm,
    out_ref,
    residual_ref, q_ref, k_ref, v_ref, gate_ref, decay_ref, offset_ref, spikes_ref, doc_ref,
    routes_ref, chosen_ref, weight_ref, gains_ref, shifts_ref,
    state_out, state_in, state_acc, decay_acc, doc_acc, mixed_ref,
    part_send, part_in, pair_send, pair_acc,
    meta_ref, normed_ref,
    outgoing, rows_ref, partial, gate_up, down, hidden, pair_in, far_out, far_in, final, returned,
    load_sems, state_send_sem, state_recv_sem, part_send_sem, part_recv_sem, pair_sems,
    weight_sems, a_send, a_recv, y_send, y_recv, p_send, p_recv,
    r_send, r_recv, f_send, f_recv, b_send, b_recv,
):
    here = lax.axis_index("sp")
    me = lax.axis_index("tp")
    core = me % 2
    side = me // 2
    partner = side * 2 + (1 - core)
    across = (1 - side) * 2 + core
    diagonal = (1 - side) * 2 + (1 - core)
    rows = q_ref.shape[0]
    lanes = q_ref.shape[1]
    key_dim = lanes // heads
    value_dim = v_ref.shape[1] // heads
    tokens, width = residual_ref.shape
    slot_total = sp_count * cap
    tile = 128
    tiles = w_gate_hbm.shape[2] // tile
    group = 2 * tp_count * cap

    loads = [
        pltpu.make_async_copy(source, target, load_sems.at[n])
        for n, (source, target) in enumerate(
            (
                (decay_hbm, decay_ref), (offset_hbm, offset_ref), (spikes_hbm, spikes_ref),
                (doc_hbm, doc_ref), (q_hbm, q_ref), (k_hbm, k_ref), (v_hbm, v_ref),
                (routes_hbm, routes_ref), (chosen_hbm, chosen_ref), (gate_hbm, gate_ref),
                (weight_hbm, weight_ref), (residual_hbm, residual_ref), (gains_hbm, gains_ref),
                (shifts_hbm, shifts_ref),
            )
        )
    ]
    for copy in loads:
        copy.start()

    barrier = pltpu.get_barrier_semaphore()

    def greet(k, carry):
        @pl.when(k != here)
        def _():
            pl.semaphore_signal(barrier, inc=1, device_id={"sp": k}, device_id_type=MESH)
        return carry

    lax.fori_loop(0, sp_count, greet, 0)
    pl.semaphore_signal(barrier, inc=1, device_id={"tp": partner}, device_id_type=MESH)
    pl.semaphore_signal(barrier, inc=1, device_id={"tp": across}, device_id_type=MESH)

    for copy in loads[:9]:
        copy.wait()

    weight_copies = []
    for j in range(tiles):
        for kind, source in enumerate((w_gate_hbm, w_up_hbm)):
            weight_copies.append(
                pltpu.make_async_copy(
                    source.at[0, :, pl.ds(j * tile, tile)],
                    gate_up.at[j, :, pl.ds(kind * tile, tile)],
                    weight_sems.at[2 * j + kind],
                )
            )
    weight_copies.append(pltpu.make_async_copy(w_down_hbm.at[0], down, weight_sems.at[2 * tiles]))
    for copy in weight_copies:
        copy.start()

    x = decay_ref[...].astype(jnp.float32) + offset_ref[...]
    rate = (jnp.minimum(x, 0.0) - jnp.log1p(jnp.exp(-jnp.abs(x)))) * (1.0 / 16.0)
    extra = jnp.concatenate(
        [jnp.broadcast_to(spikes_ref[h : h + 1, :], (key_dim, rows)) for h in range(heads)], axis=0
    ).T
    doc_row = doc_ref[...].astype(jnp.float32)
    meta_rows = [routes_ref[j : j + 1, :].astype(jnp.float32) for j in range(2)]
    meta_rows += [chosen_ref[j : j + 1, :] for j in range(2)]
    meta = jnp.concatenate(
        [jnp.broadcast_to(row, (16, rows)) for row in meta_rows]
        + [jnp.broadcast_to(doc_row, (lanes - 64, rows))],
        axis=0,
    ).T
    meta_ref[...] = meta
    doc_col = meta[:, 64:65]
    totals = rate + extra
    row_of = lax.broadcasted_iota(jnp.int32, rate.shape, 0)
    step = 1
    while step < rows:
        totals = totals + jnp.where(row_of >= step, pltpu.roll(totals, step, 0), 0.0)
        step *= 2
    last_total = totals[rows - 1 : rows, :]
    last_doc = doc_row[:, rows - 1 : rows]
    key = k_ref[...].astype(jnp.float32)
    query = q_ref[...].astype(jnp.float32) * key_dim ** (-0.5)
    ends = (key * jnp.exp(last_total - totals) * (doc_col == last_doc).astype(jnp.float32)).astype(
        jnp.bfloat16
    )
    values = v_ref[...]
    state = jnp.concatenate(
        [
            lax.dot_general(
                values[:, h * value_dim : (h + 1) * value_dim],
                ends[:, h * key_dim : (h + 1) * key_dim],
                TN,
                preferred_element_type=jnp.float32,
            )
            for h in range(heads)
        ],
        axis=1,
    )
    state_out[0:value_dim, :] = state.astype(jnp.bfloat16)
    tail_shape = (state_out.shape[0] - value_dim, lanes)
    tail_row = lax.broadcasted_iota(jnp.int32, tail_shape, 0)
    state_out[value_dim:, :] = jnp.where(
        tail_row == 0, jnp.exp(last_total), jnp.broadcast_to(last_doc, tail_shape)
    ).astype(jnp.bfloat16)
    pl.semaphore_wait(barrier, sp_count + 1)

    def state_copy(target, slot):
        return pltpu.make_async_remote_copy(
            src_ref=state_out,
            dst_ref=state_in.at[slot],
            send_sem=state_send_sem.at[target],
            recv_sem=state_recv_sem.at[slot],
            device_id={"sp": target},
            device_id_type=MESH,
        )

    def send_state(j, carry):
        target = sp_count - 1 - j

        @pl.when(target > here)
        def _():
            state_copy(target, here).start()
        return carry

    lax.fori_loop(0, sp_count, send_state, 0)

    t_of = lax.broadcasted_iota(jnp.int32, (rows, rows), 0)
    s_of = lax.broadcasted_iota(jnp.int32, (rows, rows), 1)
    apart = t_of ^ s_of
    visible = (t_of >= s_of) & (doc_col == doc_row)
    halves = []
    half = 1
    while half < rows:
        halves.append(half)
        half *= 2
    scaled = [(0, query.astype(jnp.bfloat16), k_ref[...])]
    for half in halves:
        fade = jnp.exp(-jnp.abs(totals - halfway_totals(totals, half)))
        scaled.append((half, (query * fade).astype(jnp.bfloat16), (key * fade).astype(jnp.bfloat16)))
    inner = []
    for h in range(heads):
        span = slice(h * key_dim, (h + 1) * key_dim)
        scores = None
        for half, q_part, k_part in scaled:
            product = lax.dot_general(
                q_part[:, span], k_part[:, span], NT, preferred_element_type=jnp.float32
            )
            scores = product if scores is None else jnp.where(apart >= half, product, scores)
        scores = jnp.where(visible, scores, 0.0).astype(jnp.bfloat16)
        inner.append(
            jnp.dot(
                scores,
                values[:, h * value_dim : (h + 1) * value_dim],
                preferred_element_type=jnp.float32,
            )
        )

    state_acc[...] = jnp.zeros_like(state_acc)
    decay_acc[...] = jnp.ones_like(decay_acc)
    doc_acc[...] = jnp.full_like(doc_acc, -1.0)

    def join(j, carry):
        k = here - 1 - j

        @pl.when(k >= 0)
        def _():
            state_copy(here, k).wait_recv()
            tail = state_in[k, value_dim:, :].astype(jnp.float32)
            doc_k = tail[1:2, :]

            @pl.when(j == 0)
            def _():
                doc_acc[...] = doc_k

            factor = jnp.where(doc_k == doc_acc[...], decay_acc[...], 0.0)
            state_acc[...] += state_in[k, 0:value_dim, :].astype(jnp.float32) * factor
            decay_acc[...] = factor * tail[0:1, :]
        return carry

    lax.fori_loop(0, sp_count, join, 0)
    for copy in loads[9:]:
        copy.wait()
    prefix = state_acc[...].astype(jnp.bfloat16)
    active = (doc_col == doc_acc[...]).astype(jnp.float32)
    entering = (query * jnp.exp(totals) * active).astype(jnp.bfloat16)
    for h in range(heads):
        span = slice(h * key_dim, (h + 1) * key_dim)
        out_span = slice(h * value_dim, (h + 1) * value_dim)
        recurrent = inner[h] + lax.dot_general(
            entering[:, span], prefix[:, span], NT, preferred_element_type=jnp.float32
        )
        scale = lax.rsqrt(jnp.mean(recurrent * recurrent, axis=-1, keepdims=True) + 1e-6)
        gate = silu(gate_ref[:, out_span].astype(jnp.float32))
        mixed_ref[:, out_span] = (recurrent * scale * gate).astype(jnp.bfloat16)

    def share(index):
        begin = pl.multiple_of(index * tokens, tokens)
        return jnp.dot(
            mixed_ref[pl.ds(begin, tokens), :], weight_ref[...], preferred_element_type=jnp.float32
        )

    def part_copy(slot):
        return pltpu.make_async_remote_copy(
            src_ref=part_send.at[slot],
            dst_ref=part_in.at[slot],
            send_sem=part_send_sem.at[slot],
            recv_sem=part_recv_sem.at[slot],
            device_id={"tp": partner},
            device_id_type=MESH,
        )

    pair_copy = pltpu.make_async_remote_copy(
        src_ref=pair_send,
        dst_ref=pair_acc,
        send_sem=pair_sems.at[0],
        recv_sem=pair_sems.at[1],
        device_id={"tp": across},
        device_id_type=MESH,
    )
    part_send[0] = share(diagonal).astype(jnp.bfloat16)
    part_copy(0).start()
    far = share(across)
    part_copy(0).wait_recv()
    pair_send[...] = (far + part_in[0].astype(jnp.float32)).astype(jnp.bfloat16)
    pair_copy.start()
    part_send[1] = share(partner).astype(jnp.bfloat16)
    part_copy(1).start()
    near = share(me) + residual_ref[...].astype(jnp.float32)

    begin = pl.multiple_of(me * tokens, tokens)
    own_meta = meta_ref[pl.ds(begin, tokens), :]
    routes = [own_meta[:, 16 * j : 16 * j + 1] for j in range(2)]
    chosen = [own_meta[:, 32 + 16 * j : 33 + 16 * j] for j in range(2)]
    expert_lane = lax.broadcasted_iota(jnp.int32, (tokens, 128), 1).astype(jnp.float32)
    marks = [(routes[j] == expert_lane).astype(jnp.float32) for j in range(2)]
    earlier = (
        lax.broadcasted_iota(jnp.int32, (tokens, tokens), 0)
        > lax.broadcasted_iota(jnp.int32, (tokens, tokens), 1)
    ).astype(jnp.float32)
    before = jnp.dot(
        earlier.astype(jnp.bfloat16),
        (marks[0] + marks[1]).astype(jnp.bfloat16),
        preferred_element_type=jnp.float32,
    )
    slot_lane = lax.broadcasted_iota(jnp.int32, (tokens, slot_total), 1).astype(jnp.float32)
    picks = []
    for j in range(2):
        position = jnp.sum(before * marks[j], axis=1, keepdims=True)
        slot = routes[j] * float(cap) + position
        picks.append((slot_lane == slot).astype(jnp.bfloat16))

    part_copy(1).wait_recv()
    near = near + part_in[1].astype(jnp.float32)
    pair_copy.wait_recv()
    near = near + pair_acc[...].astype(jnp.float32)
    normed_ref[...] = norm_rows(near, gains_ref[0:1, :], shifts_ref[0:1, :]).astype(jnp.bfloat16)
    outgoing[...] = lax.dot_general(
        picks[0] + picks[1], normed_ref[...], TN, preferred_element_type=jnp.float32
    ).astype(jnp.bfloat16)

    def block(ref, index):
        return ref.at[pl.ds(pl.multiple_of(index * cap, cap), cap), :]

    def load(ref, index):
        return ref[pl.ds(pl.multiple_of(index * cap, cap), cap), :]

    def remote(src, dst, send_sem, recv_sem, target):
        return pltpu.make_async_remote_copy(
            src_ref=src, dst_ref=dst, send_sem=send_sem, recv_sem=recv_sem,
            device_id=target, device_id_type=MESH,
        )

    def row_block(source, part):
        return block(rows_ref, source * tp_count + part)

    def dispatch(target, source):
        return remote(
            block(outgoing, target), row_block(source, me), a_send.at[target], a_recv.at[source],
            {"sp": target},
        )

    def to_across(source, part):
        return remote(
            row_block(source, part), row_block(source, part), y_send.at[source], y_recv.at[source],
            {"tp": across},
        )

    def to_partner(source, turn, part):
        return remote(
            row_block(source, part), row_block(source, part),
            p_send.at[source, turn], p_recv.at[source, turn], {"tp": partner},
        )

    def part_to_partner(source, turn):
        part = partner if turn == 0 else diagonal
        return remote(
            block(partial, source * tp_count + part), block(pair_in, source * 2 + turn),
            r_send.at[source, turn], r_recv.at[source, turn], {"tp": partner},
        )

    def pair_to_across(source):
        return remote(
            block(far_out, source), block(far_in, source), f_send.at[source], f_recv.at[source],
            {"tp": across},
        )

    def give_back(source, expert):
        return remote(
            block(final, source), block(returned, expert), b_send.at[source], b_recv.at[expert],
            {"sp": source},
        )

    chain = here // 2
    upper = chain // 2
    levels = (chain, flipped(chain, 1), 2 - upper, 3 - 3 * upper)

    def sources_of(i):
        base = levels[i] * 2
        return (base + here % 2, base + 1 - here % 2)

    own = pl.multiple_of((here * tp_count + me) * cap, cap)
    rows_ref[pl.ds(own, cap), :] = load(outgoing, here)
    for i in range(4):
        for n, target in enumerate(sources_of(i)):
            if i or n:
                dispatch(target, here).start()

    def spread(i, n):
        source = sources_of(i)[n]
        if i or n:
            dispatch(source, source).wait_recv()
        to_across(source, me).start()
        to_partner(source, 0, me).start()

    def relay(i, n):
        source = sources_of(i)[n]
        to_across(source, across).wait_recv()
        to_partner(source, 1, across).start()

    def compute(i):
        for source in sources_of(i):
            to_partner(source, 0, partner).wait_recv()
            to_partner(source, 1, diagonal).wait_recv()
        if i == 0:
            for copy in weight_copies:
                copy.wait()
        base = pl.multiple_of(levels[i] * group, group)

        def first(j, carry):
            both = jnp.dot(
                rows_ref[pl.ds(base, group), :], gate_up[j], preferred_element_type=jnp.float32
            )
            unit = (silu(both[:, :tile]) * both[:, tile:]).astype(jnp.bfloat16)
            hidden[:, pl.ds(pl.multiple_of(j * tile, tile), tile)] = unit
            return carry

        lax.fori_loop(0, tiles, first, 0)
        span = 512

        def second(j, carry):
            columns = pl.ds(pl.multiple_of(j * span, span), span)
            partial[pl.ds(base, group), columns] = jnp.dot(
                hidden[...], down[:, columns], preferred_element_type=jnp.float32
            ).astype(jnp.bfloat16)
            return carry

        lax.fori_loop(0, width // span, second, 0)
        for turn in (1, 0):
            for source in sources_of(i):
                part_to_partner(source, turn).start()

    def fold(i, n):
        source = sources_of(i)[n]
        part_to_partner(source, 1).wait_recv()
        far_out[pl.ds(pl.multiple_of(source * cap, cap), cap), :] = (
            load(partial, source * tp_count + across).astype(jnp.float32)
            + load(pair_in, source * 2 + 1).astype(jnp.float32)
        ).astype(jnp.bfloat16)
        pair_to_across(source).start()

    def finish(i, n):
        source = sources_of(i)[n]
        part_to_partner(source, 0).wait_recv()
        pair_to_across(source).wait_recv()
        value = (
            load(partial, source * tp_count + me).astype(jnp.float32)
            + load(pair_in, source * 2).astype(jnp.float32)
            + load(far_in, source).astype(jnp.float32)
        ).astype(jnp.bfloat16)
        if i or n:
            final[pl.ds(pl.multiple_of(source * cap, cap), cap), :] = value
            give_back(source, here).start()
        else:
            returned[pl.ds(pl.multiple_of(source * cap, cap), cap), :] = value

    stages = {"S": spread, "R": relay, "F": fold, "E": finish, "C": compute}

    def run(order):
        for item in order:
            stages[item[0]](*[int(digit) for digit in item[1:]])

    @pl.when(chain % 3 == 0)
    def _():
        run(END_ORDER)

    @pl.when(chain % 3 != 0)
    def _():
        run(INNER_ORDER)

    for i in range(4):
        for n, expert in enumerate(sources_of(i)):
            if i or n:
                give_back(here, expert).wait_recv()
    mix = chosen[0] * jnp.dot(picks[0], returned[...], preferred_element_type=jnp.float32)
    mix = mix + chosen[1] * jnp.dot(picks[1], returned[...], preferred_element_type=jnp.float32)
    out_ref[...] = norm_rows(
        normed_ref[...].astype(jnp.float32) + mix, gains_ref[1:2, :], shifts_ref[1:2, :]
    ).astype(jnp.bfloat16)

    part_copy(0).wait_send()
    part_copy(1).wait_send()
    pair_copy.wait_send()

    def drain(source, carry):
        @pl.when(source > here)
        def _():
            state_copy(source, here).wait_send()

        to_across(source, me).wait_send()
        to_partner(source, 0, me).wait_send()
        to_partner(source, 1, across).wait_send()
        part_to_partner(source, 0).wait_send()
        part_to_partner(source, 1).wait_send()
        pair_to_across(source).wait_send()

        @pl.when(source != here)
        def _():
            dispatch(source, here).wait_send()
            give_back(source, here).wait_send()
        return carry

    lax.fori_loop(0, sp_count, drain, 0)


def layer(
    sp_count, tp_count, cap, residual, q, k, v, gate, decay_in, offset, spikes, documents, weight,
    gains, shifts, routes, chosen, w_gate, w_up, w_down,
):
    rows, heads = spikes.shape
    tokens, width = residual.shape
    channels = q.shape[1]
    units = w_gate.shape[2]
    slots = sp_count * cap
    state_rows = v.shape[1] // heads + 16
    bf16, f32 = jnp.bfloat16, jnp.float32
    dma = pltpu.SemaphoreType.DMA
    inputs = (
        residual, q, k, v, gate, decay_in, offset.reshape(1, -1), spikes.T,
        documents.reshape(1, -1), routes.T, chosen.T, weight, gains, shifts, w_gate, w_up, w_down,
    )
    return pl.pallas_call(
        functools.partial(layer_kernel, heads, sp_count, tp_count, cap),
        out_shape=jax.ShapeDtypeStruct((tokens, width), bf16),
        in_specs=[pl.BlockSpec(memory_space=pltpu.HBM)] * len(inputs),
        out_specs=VMEM,
        scratch_shapes=[pltpu.VMEM(value.shape, value.dtype) for value in inputs[:14]]
        + [
            pltpu.VMEM((state_rows, channels), bf16),
            pltpu.VMEM((sp_count, state_rows, channels), bf16),
            pltpu.VMEM((state_rows - 16, channels), f32),
            pltpu.VMEM((1, channels), f32),
            pltpu.VMEM((1, channels), f32),
            pltpu.VMEM((rows, v.shape[1]), bf16),
            pltpu.VMEM((2, tokens, width), bf16),
            pltpu.VMEM((2, tokens, width), bf16),
            pltpu.VMEM((tokens, width), bf16),
            pltpu.VMEM((tokens, width), bf16),
            pltpu.VMEM((rows, channels), f32),
            pltpu.VMEM((tokens, width), bf16),
            pltpu.VMEM((slots, width), bf16),
            pltpu.VMEM((slots * tp_count, width), bf16),
            pltpu.VMEM((slots * tp_count, width), bf16),
            pltpu.VMEM((units // 128, width, 256), bf16),
            pltpu.VMEM((units, width), bf16),
            pltpu.VMEM((2 * tp_count * cap, units), bf16),
            pltpu.VMEM((slots * 2, width), bf16),
            pltpu.VMEM((slots, width), bf16),
            pltpu.VMEM((slots, width), bf16),
            pltpu.VMEM((slots, width), bf16),
            pltpu.VMEM((slots, width), bf16),
            dma((14,)),
            dma((sp_count,)),
            dma((sp_count,)),
            dma((2,)),
            dma((2,)),
            dma((2,)),
            dma((2 * (units // 128) + 1,)),
            dma((sp_count,)),
            dma((sp_count,)),
            dma((sp_count,)),
            dma((sp_count,)),
            dma((sp_count, 2)),
            dma((sp_count, 2)),
            dma((sp_count, 2)),
            dma((sp_count, 2)),
            dma((sp_count,)),
            dma((sp_count,)),
            dma((sp_count,)),
            dma((sp_count,)),
        ],
        compiler_params=pltpu.CompilerParams(
            collective_id=1, has_side_effects=True, vmem_limit_bytes=67043328
        ),
        name="layer",
    )(*inputs)


def slot_index(route_rows, block_rows, capacity, expert_count):
    row_total, top_count = route_rows.shape
    sources = row_total // block_rows
    flat_routes = route_rows.reshape(sources, block_rows * top_count)
    expert_marks = (
        flat_routes[:, :, None] == lax.broadcasted_iota(jnp.int32, (1, 1, expert_count), 2)
    ).astype(jnp.int32)
    before = jnp.cumsum(expert_marks, axis=1) - expert_marks
    position = jnp.sum(before * expert_marks, axis=2)
    source_id = lax.broadcasted_iota(jnp.int32, position.shape, 0)
    slots = flat_routes * (sources * capacity) + source_id * capacity + position
    return slots.reshape(row_total, top_count)


def fill_slots(row_block, slots, slot_total):
    owners = lax.broadcasted_iota(jnp.int32, slots.shape, 0).reshape(-1)
    slot_owner = (
        jnp.full((slot_total,), slots.shape[0], jnp.int32).at[slots.reshape(-1)].set(owners)
    )
    return jnp.take(row_block, slot_owner, axis=0, mode="fill", fill_value=0)


def expert_quarter(row_block, gate_part, up_part, down_part):
    gate_val = jnp.dot(row_block, gate_part, preferred_element_type=jnp.float32)
    up_val = jnp.dot(row_block, up_part, preferred_element_type=jnp.float32)
    hidden = (jax.nn.silu(gate_val) * up_val).astype(jnp.bfloat16)
    return jnp.dot(hidden, down_part, preferred_element_type=jnp.float32).astype(jnp.bfloat16)


def combine_rows(returned, slots, weight_rows):
    model_width = returned.shape[-1]
    picked = jnp.take(returned.reshape(-1, model_width), slots.reshape(-1), axis=0)
    picked = picked.reshape(slots.shape + (model_width,))
    return jnp.sum(picked * weight_rows[:, :, None], axis=1)


def on_device(
    residual,
    queries,
    projected_keys,
    values,
    projected_output_gate,
    decay_gate_input,
    decay_gate_offset,
    decay_spikes,
    documents,
    attention_output_weight,
    layer_norm_gains,
    layer_norm_shifts,
    routes,
    chosen_expert_weights,
    expert_gate_weight,
    expert_up_weight,
    expert_down_weight,
):
    sequence_length, head_number = decay_spikes.shape
    rows_dev, model_width = residual.shape
    expert_count = lax.axis_size("sp")
    capacity = max(2, 4 * rows_dev // expert_count)
    peers, parts = lax.axis_size("sp"), lax.axis_size("tp")
    channels = queries.shape[1]
    if (
        capacity % 16 == 0 and peers == 8 and parts == 4 and channels == 128
        and sequence_length % 128 == 0
    ):
        return layer(
            peers, parts, capacity, residual, queries, projected_keys, values,
            projected_output_gate, decay_gate_input, decay_gate_offset, decay_spikes, documents,
            attention_output_weight, layer_norm_gains, layer_norm_shifts, routes,
            chosen_expert_weights, expert_gate_weight, expert_up_weight, expert_down_weight,
        )
    normed = attention(
        peers, parts, residual, queries, projected_keys, values,
        projected_output_gate, decay_gate_input, decay_gate_offset, decay_spikes, documents,
        attention_output_weight, layer_norm_gains, layer_norm_shifts,
    )
    own_routes = lax.dynamic_slice_in_dim(routes, lax.axis_index("tp") * rows_dev, rows_dev, 0)
    own_weights = lax.dynamic_slice_in_dim(
        chosen_expert_weights, lax.axis_index("tp") * rows_dev, rows_dev, 0
    )
    slots = slot_index(own_routes, rows_dev, capacity, expert_count)
    outgoing = fill_slots(normed, slots, expert_count * capacity).reshape(
        expert_count, capacity, model_width
    )
    all_rows = lax.all_gather(
        lax.all_to_all(outgoing, "sp", split_axis=0, concat_axis=0, tiled=True),
        "tp",
        axis=1,
        tiled=True,
    )
    sources, slot_count, _ = all_rows.shape
    partial_value = expert_quarter(
        all_rows.reshape(sources * slot_count, model_width),
        expert_gate_weight[0],
        expert_up_weight[0],
        expert_down_weight[0],
    )
    summed = lax.psum_scatter(
        partial_value.reshape(sources, slot_count, model_width)
        .astype(jnp.float32)
        .astype(jnp.bfloat16),
        "tp",
        scatter_dimension=1,
        tiled=True,
    ).astype(jnp.float32)
    returned = lax.all_to_all(
        summed.astype(jnp.bfloat16), "sp", split_axis=0, concat_axis=0, tiled=True
    ).astype(summed.dtype)
    expert_mix = combine_rows(returned, slots, own_weights)
    return norm_rows(
        normed.astype(jnp.float32) + expert_mix, layer_norm_gains[1], layer_norm_shifts[1]
    ).astype(jnp.bfloat16)


def solution(mesh):
    placed = (
        P(("sp", "tp"), None),
        P("sp", "tp"),
        P("sp", "tp"),
        P("sp", "tp"),
        P("sp", "tp"),
        P("sp", "tp"),
        P("tp"),
        P("sp", "tp"),
        P("sp"),
        P("tp", None),
        P(),
        P(),
        P("sp", None),
        P("sp", None),
        P("sp", None, "tp"),
        P("sp", None, "tp"),
        P("sp", "tp", None),
    )
    return jax.shard_map(
        on_device, mesh=mesh, in_specs=placed, out_specs=P(("sp", "tp"), None), check_vma=False
    )
```

```python
import functools
import jax
import jax.numpy as jnp
from jax import lax
from jax.experimental import pallas as pl
from jax.experimental.pallas import tpu as pltpu
from jax.sharding import PartitionSpec as P

MESH = pl.DeviceIdType.MESH
VMEM = pl.BlockSpec(memory_space=pltpu.VMEM)
NT = (((1,), (1,)), ((), ()))
TN = (((0,), (0,)), ((), ()))


def silu(v):
    return v / (1.0 + jnp.exp(-v))


def halfway_totals(totals, half):
    rows, width = totals.shape
    if half >= 4:
        grouped = totals.reshape(rows // (2 * half), 2 * half, width)
        return jnp.broadcast_to(grouped[:, half - 1 : half, :], grouped.shape).reshape(rows, width)
    row = lax.broadcasted_iota(jnp.int32, totals.shape, 0) % (2 * half)
    found = totals
    for place in range(2 * half):
        shift = place - (half - 1)
        if shift:
            found = jnp.where(row == place, pltpu.roll(totals, shift % rows, 0), found)
    return found


def attention_kernel(
    heads, sp_count, tp_count,
    q_ref, k_ref, v_ref, gate_ref, decay_ref, offset_ref, spikes_ref, doc_col_ref, doc_row_ref,
    weight_ref, residual_ref, gains_ref, shifts_ref,
    normed_ref,
    state_out, state_in, state_acc, decay_acc, doc_acc, mixed_ref,
    part_send, part_in, pair_send, pair_in,
    state_send_sem, state_recv_sem, part_send_sem, part_recv_sem, pair_sems,
):
    here = lax.axis_index("sp")
    me = lax.axis_index("tp")
    core = me % 2
    side = me // 2
    partner = side * 2 + (1 - core)
    across = (1 - side) * 2 + core
    rows = q_ref.shape[0]
    key_dim = q_ref.shape[1] // heads
    value_dim = v_ref.shape[1] // heads
    own_rows = residual_ref.shape[0]

    barrier = pltpu.get_barrier_semaphore()

    def greet(k, carry):
        @pl.when(k != here)
        def _():
            pl.semaphore_signal(barrier, inc=1, device_id={"sp": k}, device_id_type=MESH)
        return carry

    lax.fori_loop(0, sp_count, greet, 0)
    pl.semaphore_signal(barrier, inc=1, device_id={"tp": partner}, device_id_type=MESH)
    pl.semaphore_signal(barrier, inc=1, device_id={"tp": across}, device_id_type=MESH)

    x = decay_ref[...].astype(jnp.float32) + offset_ref[...]
    rate = (jnp.minimum(x, 0.0) - jnp.log1p(jnp.exp(-jnp.abs(x)))) * (1.0 / 16.0)
    lane_head = lax.broadcasted_iota(jnp.int32, rate.shape, 1) // key_dim
    spikes = spikes_ref[...]
    extra = jnp.zeros_like(rate)
    for h in range(heads):
        extra = jnp.where(lane_head == h, spikes[:, h : h + 1], extra)
    totals = rate + extra
    row_of = lax.broadcasted_iota(jnp.int32, rate.shape, 0)
    step = 1
    while step < rows:
        totals = totals + jnp.where(row_of >= step, pltpu.roll(totals, step, 0), 0.0)
        step *= 2
    doc_col = doc_col_ref[...]
    doc_row = doc_row_ref[...]
    last_total = totals[rows - 1 : rows, :]
    last_doc = doc_row[:, rows - 1 : rows]
    key = k_ref[...].astype(jnp.float32)
    query = q_ref[...].astype(jnp.float32) * key_dim ** (-0.5)
    ends = (key * jnp.exp(last_total - totals) * (doc_col == last_doc).astype(jnp.float32)).astype(
        jnp.bfloat16
    )
    values = v_ref[...]
    state = jnp.concatenate(
        [
            lax.dot_general(
                values[:, h * value_dim : (h + 1) * value_dim],
                ends[:, h * key_dim : (h + 1) * key_dim],
                TN,
                preferred_element_type=jnp.float32,
            )
            for h in range(heads)
        ],
        axis=1,
    )
    state_out[0:value_dim, :] = state.astype(jnp.bfloat16)
    tail_shape = (state_out.shape[0] - value_dim, rate.shape[1])
    tail_row = lax.broadcasted_iota(jnp.int32, tail_shape, 0)
    state_out[value_dim:, :] = jnp.where(
        tail_row == 0, jnp.exp(last_total), last_doc.astype(jnp.float32)
    ).astype(jnp.bfloat16)
    pl.semaphore_wait(barrier, sp_count + 1)

    def state_copy(target, slot):
        return pltpu.make_async_remote_copy(
            src_ref=state_out,
            dst_ref=state_in.at[slot],
            send_sem=state_send_sem.at[target],
            recv_sem=state_recv_sem.at[slot],
            device_id={"sp": target},
            device_id_type=MESH,
        )

    def send_state(j, carry):
        target = sp_count - 1 - j

        @pl.when(target > here)
        def _():
            state_copy(target, here).start()
        return carry

    lax.fori_loop(0, sp_count, send_state, 0)

    t_of = lax.broadcasted_iota(jnp.int32, (rows, rows), 0)
    s_of = lax.broadcasted_iota(jnp.int32, (rows, rows), 1)
    apart = t_of ^ s_of
    visible = (t_of >= s_of) & (doc_col == doc_row)
    halves = []
    half = 1
    while half < rows:
        halves.append(half)
        half *= 2
    scaled = [(0, query.astype(jnp.bfloat16), k_ref[...])]
    for half in halves:
        fade = jnp.exp(-jnp.abs(totals - halfway_totals(totals, half)))
        scaled.append((half, (query * fade).astype(jnp.bfloat16), (key * fade).astype(jnp.bfloat16)))
    inner = []
    for h in range(heads):
        span = slice(h * key_dim, (h + 1) * key_dim)
        scores = None
        for half, q_part, k_part in scaled:
            product = lax.dot_general(
                q_part[:, span], k_part[:, span], NT, preferred_element_type=jnp.float32
            )
            scores = product if scores is None else jnp.where(apart >= half, product, scores)
        scores = jnp.where(visible, scores, 0.0).astype(jnp.bfloat16)
        inner.append(
            jnp.dot(
                scores,
                values[:, h * value_dim : (h + 1) * value_dim],
                preferred_element_type=jnp.float32,
            )
        )

    state_acc[...] = jnp.zeros_like(state_acc)
    decay_acc[...] = jnp.ones_like(decay_acc)
    doc_acc[...] = jnp.full_like(doc_acc, -1.0)

    def join(j, carry):
        k = here - 1 - j

        @pl.when(k >= 0)
        def _():
            state_copy(here, k).wait_recv()
            tail = state_in[k, value_dim:, :].astype(jnp.float32)
            doc_k = tail[1:2, :]

            @pl.when(j == 0)
            def _():
                doc_acc[...] = doc_k

            factor = jnp.where(doc_k == doc_acc[...], decay_acc[...], 0.0)
            state_acc[...] += state_in[k, 0:value_dim, :].astype(jnp.float32) * factor
            decay_acc[...] = factor * tail[0:1, :]
        return carry

    lax.fori_loop(0, sp_count, join, 0)
    prefix = state_acc[...].astype(jnp.bfloat16)
    active = (doc_col.astype(jnp.float32) == doc_acc[...]).astype(jnp.float32)
    entering = (query * jnp.exp(totals) * active).astype(jnp.bfloat16)
    for h in range(heads):
        span = slice(h * key_dim, (h + 1) * key_dim)
        out_span = slice(h * value_dim, (h + 1) * value_dim)
        recurrent = inner[h] + lax.dot_general(
            entering[:, span], prefix[:, span], NT, preferred_element_type=jnp.float32
        )
        scale = lax.rsqrt(jnp.mean(recurrent * recurrent, axis=-1, keepdims=True) + 1e-6)
        gate = silu(gate_ref[:, out_span].astype(jnp.float32))
        mixed_ref[:, out_span] = (recurrent * scale * gate).astype(jnp.bfloat16)

    def share(index):
        begin = pl.multiple_of(index * own_rows, own_rows)
        return jnp.dot(
            mixed_ref[pl.ds(begin, own_rows), :], weight_ref[...], preferred_element_type=jnp.float32
        )

    def part_copy(slot):
        return pltpu.make_async_remote_copy(
            src_ref=part_send.at[slot],
            dst_ref=part_in.at[slot],
            send_sem=part_send_sem.at[slot],
            recv_sem=part_recv_sem.at[slot],
            device_id={"tp": partner},
            device_id_type=MESH,
        )

    pair_copy = pltpu.make_async_remote_copy(
        src_ref=pair_send,
        dst_ref=pair_in,
        send_sem=pair_sems.at[0],
        recv_sem=pair_sems.at[1],
        device_id={"tp": across},
        device_id_type=MESH,
    )
    part_send[0] = share((1 - side) * 2 + (1 - core)).astype(jnp.bfloat16)
    part_copy(0).start()
    part_send[1] = share(side * 2 + (1 - core)).astype(jnp.bfloat16)
    part_copy(1).start()
    far = share(across)
    part_copy(0).wait_recv()
    pair_send[...] = (far + part_in[0].astype(jnp.float32)).astype(jnp.bfloat16)
    pair_copy.start()
    near = share(me) + residual_ref[...].astype(jnp.float32)
    part_copy(1).wait_recv()
    near = near + part_in[1].astype(jnp.float32)
    pair_copy.wait_recv()
    near = near + pair_in[...].astype(jnp.float32)
    normed_ref[...] = norm_rows(near, gains_ref[0:1, :], shifts_ref[0:1, :]).astype(jnp.bfloat16)
    part_copy(0).wait_send()
    part_copy(1).wait_send()
    pair_copy.wait_send()

    def finish(j, carry):
        @pl.when(j > here)
        def _():
            state_copy(j, here).wait_send()
        return carry

    lax.fori_loop(0, sp_count, finish, 0)


def norm_rows(stream, gain, shift):
    center = jnp.mean(stream, axis=-1, keepdims=True)
    moved = stream - center
    spread = jnp.mean(moved * moved, axis=-1, keepdims=True)
    return moved * lax.rsqrt(spread + 1e-5) * gain + shift


def attention(sp_count, tp_count, residual, q, k, v, gate, decay_in, offset, spikes, documents, weight, gains, shifts):
    rows, heads = spikes.shape
    own_rows, width = residual.shape
    channels = q.shape[1]
    value_dim = v.shape[1] // heads
    state_rows = value_dim + 16
    return pl.pallas_call(
        functools.partial(attention_kernel, heads, sp_count, tp_count),
        out_shape=jax.ShapeDtypeStruct((own_rows, width), jnp.bfloat16),
        in_specs=[VMEM] * 13,
        out_specs=VMEM,
        scratch_shapes=[
            pltpu.VMEM((state_rows, channels), jnp.bfloat16),
            pltpu.VMEM((sp_count, state_rows, channels), jnp.bfloat16),
            pltpu.VMEM((value_dim, channels), jnp.float32),
            pltpu.VMEM((1, channels), jnp.float32),
            pltpu.VMEM((1, channels), jnp.float32),
            pltpu.VMEM((rows, v.shape[1]), jnp.bfloat16),
            pltpu.VMEM((2, own_rows, width), jnp.bfloat16),
            pltpu.VMEM((2, own_rows, width), jnp.bfloat16),
            pltpu.VMEM((own_rows, width), jnp.bfloat16),
            pltpu.VMEM((own_rows, width), jnp.bfloat16),
            pltpu.SemaphoreType.DMA((sp_count,)),
            pltpu.SemaphoreType.DMA((sp_count,)),
            pltpu.SemaphoreType.DMA((2,)),
            pltpu.SemaphoreType.DMA((2,)),
            pltpu.SemaphoreType.DMA((2,)),
        ],
        compiler_params=pltpu.CompilerParams(
            collective_id=0, has_side_effects=True, vmem_limit_bytes=48 * 1024 * 1024
        ),
        name="attention",
    )(
        q, k, v, gate, decay_in, offset.reshape(1, -1), spikes, documents.reshape(-1, 1),
        documents.reshape(1, -1), weight, residual, gains, shifts,
    )

def flipped(index, mask):
    bit, result = 1, index
    while bit <= mask:
        if mask & bit:
            result = result + bit * (1 - 2 * ((index // bit) % 2))
        bit *= 2
    return result


def flipped(index, mask):
    bit, result = 1, index
    while bit <= mask:
        if mask & bit:
            result = result + bit * (1 - 2 * ((index // bit) % 2))
        bit *= 2
    return result


END_PLAN = (
    ("D01", "D20", "D21", "S00", "S01", "R00", "S10", "D10", "D11", "R01", "W0", "D30", "D31",),
    ("S20",),
    ("S11", "R10", "S21", "R11", "S30", "W1",),
    ("S31",),
    ("F10", "F11", "R20", "R21", "W2",),
    ("R30",),
    ("R31", "F01", "W3",),
    ("E10",),
    ("F30", "F31", "E11", "F20", "F21", "F00", "E01", "E30", "E31", "E20", "E21", "E00",),
)
INNER_PLAN = (
    ("D01", "D10", "D11", "D20", "D21", "S00", "S10", "S01", "R00", "S11", "S20", "R01", "W0",
     "D30", "D31",),
    ("S21",),
    ("R10", "R11", "F01", "W1",),
    ("S30",),
    ("R20", "R21", "S31", "F10", "W2",),
    (),
    ("F20", "F21", "R30", "R31", "W3",),
    ("E01",),
    ("F30", "F31", "E20", "E21", "F11", "F00", "E10", "E30", "E31", "E11", "E00",),
)


def layer_kernel(
    heads, sp_count, tp_count, cap,
    residual_hbm, q_hbm, k_hbm, v_hbm, gate_hbm, decay_hbm, offset_hbm, spikes_hbm, doc_hbm,
    routes_hbm, chosen_hbm, weight_hbm, gains_hbm, shifts_hbm, w_gate_hbm, w_up_hbm, w_down_hbm,
    out_ref,
    residual_ref, q_ref, k_ref, v_ref, gate_ref, decay_ref, offset_ref, spikes_ref, doc_ref,
    routes_ref, chosen_ref, weight_ref, gains_ref, shifts_ref,
    state_out, state_in, state_acc, decay_acc, doc_acc, mixed_ref,
    part_send, part_in, pair_send, pair_acc,
    meta_ref, normed_ref,
    outgoing, rows_ref, partial, gate_up, down, hidden, pair_in, far_out, far_in, final, returned,
    load_sems, state_send_sem, state_recv_sem, part_send_sem, part_recv_sem, pair_sems,
    weight_sems, a_send, a_recv, y_send, y_recv, p_send, p_recv,
    r_send, r_recv, f_send, f_recv, b_send, b_recv,
):
    here = lax.axis_index("sp")
    me = lax.axis_index("tp")
    core = me % 2
    side = me // 2
    partner = side * 2 + (1 - core)
    across = (1 - side) * 2 + core
    diagonal = (1 - side) * 2 + (1 - core)
    rows = q_ref.shape[0]
    lanes = q_ref.shape[1]
    key_dim = lanes // heads
    value_dim = v_ref.shape[1] // heads
    tokens, width = residual_ref.shape
    slot_total = sp_count * cap
    tile = 128
    tiles = w_gate_hbm.shape[2] // tile
    group = 2 * tp_count * cap

    loads = [
        pltpu.make_async_copy(source, target, load_sems.at[n])
        for n, (source, target) in enumerate(
            (
                (decay_hbm, decay_ref), (offset_hbm, offset_ref), (spikes_hbm, spikes_ref),
                (doc_hbm, doc_ref), (q_hbm, q_ref), (k_hbm, k_ref), (v_hbm, v_ref),
                (routes_hbm, routes_ref), (chosen_hbm, chosen_ref), (gate_hbm, gate_ref),
                (weight_hbm, weight_ref), (residual_hbm, residual_ref), (gains_hbm, gains_ref),
                (shifts_hbm, shifts_ref),
            )
        )
    ]
    for copy in loads:
        copy.start()

    barrier = pltpu.get_barrier_semaphore()

    def greet(k, carry):
        @pl.when(k != here)
        def _():
            pl.semaphore_signal(barrier, inc=1, device_id={"sp": k}, device_id_type=MESH)
        return carry

    lax.fori_loop(0, sp_count, greet, 0)
    pl.semaphore_signal(barrier, inc=1, device_id={"tp": partner}, device_id_type=MESH)
    pl.semaphore_signal(barrier, inc=1, device_id={"tp": across}, device_id_type=MESH)

    for copy in loads[:9]:
        copy.wait()

    weight_copies = []
    for j in range(tiles):
        for kind, source in enumerate((w_gate_hbm, w_up_hbm)):
            weight_copies.append(
                pltpu.make_async_copy(
                    source.at[0, :, pl.ds(j * tile, tile)],
                    gate_up.at[j, :, pl.ds(kind * tile, tile)],
                    weight_sems.at[2 * j + kind],
                )
            )
    weight_copies.append(pltpu.make_async_copy(w_down_hbm.at[0], down, weight_sems.at[2 * tiles]))
    for copy in weight_copies:
        copy.start()

    x = decay_ref[...].astype(jnp.float32) + offset_ref[...]
    rate = (jnp.minimum(x, 0.0) - jnp.log1p(jnp.exp(-jnp.abs(x)))) * (1.0 / 16.0)
    extra = jnp.concatenate(
        [jnp.broadcast_to(spikes_ref[h : h + 1, :], (key_dim, rows)) for h in range(heads)], axis=0
    ).T
    doc_row = doc_ref[...].astype(jnp.float32)
    meta_rows = [routes_ref[j : j + 1, :].astype(jnp.float32) for j in range(2)]
    meta_rows += [chosen_ref[j : j + 1, :] for j in range(2)]
    meta = jnp.concatenate(
        [jnp.broadcast_to(row, (16, rows)) for row in meta_rows]
        + [jnp.broadcast_to(doc_row, (lanes - 64, rows))],
        axis=0,
    ).T
    meta_ref[...] = meta
    doc_col = meta[:, 64:65]
    totals = rate + extra
    row_of = lax.broadcasted_iota(jnp.int32, rate.shape, 0)
    step = 1
    while step < rows:
        totals = totals + jnp.where(row_of >= step, pltpu.roll(totals, step, 0), 0.0)
        step *= 2
    last_total = totals[rows - 1 : rows, :]
    last_doc = doc_row[:, rows - 1 : rows]
    key = k_ref[...].astype(jnp.float32)
    query = q_ref[...].astype(jnp.float32) * key_dim ** (-0.5)
    ends = (key * jnp.exp(last_total - totals) * (doc_col == last_doc).astype(jnp.float32)).astype(
        jnp.bfloat16
    )
    values = v_ref[...]
    state = jnp.concatenate(
        [
            lax.dot_general(
                values[:, h * value_dim : (h + 1) * value_dim],
                ends[:, h * key_dim : (h + 1) * key_dim],
                TN,
                preferred_element_type=jnp.float32,
            )
            for h in range(heads)
        ],
        axis=1,
    )
    state_out[0:value_dim, :] = state.astype(jnp.bfloat16)
    tail_shape = (state_out.shape[0] - value_dim, lanes)
    tail_row = lax.broadcasted_iota(jnp.int32, tail_shape, 0)
    state_out[value_dim:, :] = jnp.where(
        tail_row == 0, jnp.exp(last_total), jnp.broadcast_to(last_doc, tail_shape)
    ).astype(jnp.bfloat16)
    begin = pl.multiple_of(me * tokens, tokens)
    own_meta = meta_ref[pl.ds(begin, tokens), :]
    routes = [own_meta[:, 16 * j : 16 * j + 1] for j in range(2)]
    chosen = [own_meta[:, 32 + 16 * j : 33 + 16 * j] for j in range(2)]
    expert_lane = lax.broadcasted_iota(jnp.int32, (tokens, 128), 1).astype(jnp.float32)
    marks = [(routes[j] == expert_lane).astype(jnp.float32) for j in range(2)]
    earlier = (
        lax.broadcasted_iota(jnp.int32, (tokens, tokens), 0)
        > lax.broadcasted_iota(jnp.int32, (tokens, tokens), 1)
    ).astype(jnp.float32)
    before = jnp.dot(
        earlier.astype(jnp.bfloat16),
        (marks[0] + marks[1]).astype(jnp.bfloat16),
        preferred_element_type=jnp.float32,
    )
    slot_lane = lax.broadcasted_iota(jnp.int32, (tokens, slot_total), 1).astype(jnp.float32)
    picks = []
    for j in range(2):
        position = jnp.sum(before * marks[j], axis=1, keepdims=True)
        slot = routes[j] * float(cap) + position
        picks.append((slot_lane == slot).astype(jnp.bfloat16))

    pl.semaphore_wait(barrier, sp_count + 1)

    def state_copy(target, slot):
        return pltpu.make_async_remote_copy(
            src_ref=state_out,
            dst_ref=state_in.at[slot],
            send_sem=state_send_sem.at[target],
            recv_sem=state_recv_sem.at[slot],
            device_id={"sp": target},
            device_id_type=MESH,
        )

    def send_state(j, carry):
        target = sp_count - 1 - j

        @pl.when(target > here)
        def _():
            state_copy(target, here).start()
        return carry

    lax.fori_loop(0, sp_count, send_state, 0)

    t_of = lax.broadcasted_iota(jnp.int32, (rows, rows), 0)
    s_of = lax.broadcasted_iota(jnp.int32, (rows, rows), 1)
    apart = t_of ^ s_of
    visible = (t_of >= s_of) & (doc_col == doc_row)
    halves = []
    half = 1
    while half < rows:
        halves.append(half)
        half *= 2
    scaled = [(0, query.astype(jnp.bfloat16), k_ref[...])]
    for half in halves:
        fade = jnp.exp(-jnp.abs(totals - halfway_totals(totals, half)))
        scaled.append((half, (query * fade).astype(jnp.bfloat16), (key * fade).astype(jnp.bfloat16)))
    inner = []
    for h in range(heads):
        span = slice(h * key_dim, (h + 1) * key_dim)
        scores = None
        for half, q_part, k_part in scaled:
            product = lax.dot_general(
                q_part[:, span], k_part[:, span], NT, preferred_element_type=jnp.float32
            )
            scores = product if scores is None else jnp.where(apart >= half, product, scores)
        scores = jnp.where(visible, scores, 0.0).astype(jnp.bfloat16)
        inner.append(
            jnp.dot(
                scores,
                values[:, h * value_dim : (h + 1) * value_dim],
                preferred_element_type=jnp.float32,
            )
        )

    state_acc[...] = jnp.zeros_like(state_acc)
    decay_acc[...] = jnp.ones_like(decay_acc)
    doc_acc[...] = jnp.full_like(doc_acc, -1.0)

    def join(j, carry):
        k = here - 1 - j

        @pl.when(k >= 0)
        def _():
            state_copy(here, k).wait_recv()
            tail = state_in[k, value_dim:, :].astype(jnp.float32)
            doc_k = tail[1:2, :]

            @pl.when(j == 0)
            def _():
                doc_acc[...] = doc_k

            factor = jnp.where(doc_k == doc_acc[...], decay_acc[...], 0.0)
            state_acc[...] += state_in[k, 0:value_dim, :].astype(jnp.float32) * factor
            decay_acc[...] = factor * tail[0:1, :]
        return carry

    lax.fori_loop(0, sp_count, join, 0)
    for copy in loads[9:]:
        copy.wait()
    prefix = state_acc[...].astype(jnp.bfloat16)
    active = (doc_col == doc_acc[...]).astype(jnp.float32)
    entering = (query * jnp.exp(totals) * active).astype(jnp.bfloat16)
    for h in range(heads):
        span = slice(h * key_dim, (h + 1) * key_dim)
        out_span = slice(h * value_dim, (h + 1) * value_dim)
        recurrent = inner[h] + lax.dot_general(
            entering[:, span], prefix[:, span], NT, preferred_element_type=jnp.float32
        )
        scale = lax.rsqrt(jnp.mean(recurrent * recurrent, axis=-1, keepdims=True) + 1e-6)
        gate = silu(gate_ref[:, out_span].astype(jnp.float32))
        mixed_ref[:, out_span] = (recurrent * scale * gate).astype(jnp.bfloat16)

    def share(index):
        begin = pl.multiple_of(index * tokens, tokens)
        return jnp.dot(
            mixed_ref[pl.ds(begin, tokens), :], weight_ref[...], preferred_element_type=jnp.float32
        )

    def part_copy(slot):
        return pltpu.make_async_remote_copy(
            src_ref=part_send.at[slot],
            dst_ref=part_in.at[slot],
            send_sem=part_send_sem.at[slot],
            recv_sem=part_recv_sem.at[slot],
            device_id={"tp": partner},
            device_id_type=MESH,
        )

    pair_copy = pltpu.make_async_remote_copy(
        src_ref=pair_send,
        dst_ref=pair_acc,
        send_sem=pair_sems.at[0],
        recv_sem=pair_sems.at[1],
        device_id={"tp": across},
        device_id_type=MESH,
    )
    part_send[0] = share(diagonal).astype(jnp.bfloat16)
    part_copy(0).start()
    far = share(across)
    part_copy(0).wait_recv()
    pair_send[...] = (far + part_in[0].astype(jnp.float32)).astype(jnp.bfloat16)
    pair_copy.start()
    part_send[1] = share(partner).astype(jnp.bfloat16)
    part_copy(1).start()
    near = share(me) + residual_ref[...].astype(jnp.float32)

    part_copy(1).wait_recv()
    near = near + part_in[1].astype(jnp.float32)
    pair_copy.wait_recv()
    near = near + pair_acc[...].astype(jnp.float32)
    normed_ref[...] = norm_rows(near, gains_ref[0:1, :], shifts_ref[0:1, :]).astype(jnp.bfloat16)
    outgoing[...] = lax.dot_general(
        picks[0] + picks[1], normed_ref[...], TN, preferred_element_type=jnp.float32
    ).astype(jnp.bfloat16)

    def block(ref, index):
        return ref.at[pl.ds(pl.multiple_of(index * cap, cap), cap), :]

    def load(ref, index):
        return ref[pl.ds(pl.multiple_of(index * cap, cap), cap), :]

    def remote(src, dst, send_sem, recv_sem, target):
        return pltpu.make_async_remote_copy(
            src_ref=src, dst_ref=dst, send_sem=send_sem, recv_sem=recv_sem,
            device_id=target, device_id_type=MESH,
        )

    def row_block(source, part):
        return block(rows_ref, source * tp_count + part)

    def dispatch(target, source):
        return remote(
            block(outgoing, target), row_block(source, me), a_send.at[target], a_recv.at[source],
            {"sp": target},
        )

    def to_across(source, part):
        return remote(
            row_block(source, part), row_block(source, part), y_send.at[source], y_recv.at[source],
            {"tp": across},
        )

    def to_partner(source, turn, part):
        return remote(
            row_block(source, part), row_block(source, part),
            p_send.at[source, turn], p_recv.at[source, turn], {"tp": partner},
        )

    def part_to_partner(source, turn):
        part = partner if turn == 0 else diagonal
        return remote(
            block(partial, source * tp_count + part), block(pair_in, source * 2 + turn),
            r_send.at[source, turn], r_recv.at[source, turn], {"tp": partner},
        )

    def pair_to_across(source):
        return remote(
            block(far_out, source), block(far_in, source), f_send.at[source], f_recv.at[source],
            {"tp": across},
        )

    def give_back(source, expert):
        return remote(
            block(final, source), block(returned, expert), b_send.at[source], b_recv.at[expert],
            {"sp": source},
        )

    chain = here // 2
    upper = chain // 2
    near, inner_far, end_far = flipped(chain, 1), 2 - upper, 3 - 3 * upper
    at_end = chain % 3 == 0
    ending = at_end.astype(jnp.int32)
    levels = (
        chain,
        near + ending * (inner_far - near),
        end_far + ending * (near - end_far),
        inner_far + ending * (end_far - inner_far),
    )

    def sources_of(i):
        base = levels[i] * 2
        return (base + here % 2, base + 1 - here % 2)

    own = pl.multiple_of((here * tp_count + me) * cap, cap)
    rows_ref[pl.ds(own, cap), :] = load(outgoing, here)

    def send(i, n):
        dispatch(sources_of(i)[n], here).start()

    def spread(i, n):
        source = sources_of(i)[n]
        if i or n:
            dispatch(source, source).wait_recv()
        to_across(source, me).start()
        to_partner(source, 0, me).start()

    def relay(i, n):
        source = sources_of(i)[n]
        to_across(source, across).wait_recv()
        to_partner(source, 1, across).start()

    def gathered(i):
        for source in sources_of(i):
            to_partner(source, 0, partner).wait_recv()
            to_partner(source, 1, diagonal).wait_recv()

    def compute(i):
        base = pl.multiple_of(levels[i] * group, group)

        def first(j, carry):
            both = jnp.dot(
                rows_ref[pl.ds(base, group), :], gate_up[j], preferred_element_type=jnp.float32
            )
            unit = (silu(both[:, :tile]) * both[:, tile:]).astype(jnp.bfloat16)
            hidden[:, pl.ds(pl.multiple_of(j * tile, tile), tile)] = unit
            return carry

        lax.fori_loop(0, tiles, first, 0, unroll=True)

    def project(i):
        base = pl.multiple_of(levels[i] * group, group)
        span = 512

        def second(j, carry):
            columns = pl.ds(pl.multiple_of(j * span, span), span)
            partial[pl.ds(base, group), columns] = jnp.dot(
                hidden[...], down[:, columns], preferred_element_type=jnp.float32
            ).astype(jnp.bfloat16)
            return carry

        lax.fori_loop(0, width // span, second, 0, unroll=True)
        for turn in (1, 0):
            for source in sources_of(i):
                part_to_partner(source, turn).start()

    def fold(i, n):
        source = sources_of(i)[n]
        part_to_partner(source, 1).wait_recv()
        far_out[pl.ds(pl.multiple_of(source * cap, cap), cap), :] = (
            load(partial, source * tp_count + across).astype(jnp.float32)
            + load(pair_in, source * 2 + 1).astype(jnp.float32)
        ).astype(jnp.bfloat16)
        pair_to_across(source).start()

    def finish(i, n):
        source = sources_of(i)[n]
        part_to_partner(source, 0).wait_recv()
        pair_to_across(source).wait_recv()
        value = (
            load(partial, source * tp_count + me).astype(jnp.float32)
            + load(pair_in, source * 2).astype(jnp.float32)
            + load(far_in, source).astype(jnp.float32)
        ).astype(jnp.bfloat16)
        if i or n:
            final[pl.ds(pl.multiple_of(source * cap, cap), cap), :] = value
            give_back(source, here).start()
        else:
            returned[pl.ds(pl.multiple_of(source * cap, cap), cap), :] = value

    stages = {"D": send, "S": spread, "R": relay, "W": gathered, "F": fold, "E": finish}

    def run(order):
        for item in order:
            stages[item[0]](*[int(digit) for digit in item[1:]])

    for copy in weight_copies:
        copy.wait()
    for i in range(9):
        if END_PLAN[i]:
            pl.when(at_end)(functools.partial(run, END_PLAN[i]))
        if INNER_PLAN[i]:
            pl.when(jnp.logical_not(at_end))(functools.partial(run, INNER_PLAN[i]))
        if i < 8:
            (project if i % 2 else compute)(i // 2)

    for i in range(4):
        for n, expert in enumerate(sources_of(i)):
            if i or n:
                give_back(here, expert).wait_recv()
    mix = chosen[0] * jnp.dot(picks[0], returned[...], preferred_element_type=jnp.float32)
    mix = mix + chosen[1] * jnp.dot(picks[1], returned[...], preferred_element_type=jnp.float32)
    out_ref[...] = norm_rows(
        normed_ref[...].astype(jnp.float32) + mix, gains_ref[1:2, :], shifts_ref[1:2, :]
    ).astype(jnp.bfloat16)

    part_copy(0).wait_send()
    part_copy(1).wait_send()
    pair_copy.wait_send()

    def drain(source, carry):
        @pl.when(source > here)
        def _():
            state_copy(source, here).wait_send()

        to_across(source, me).wait_send()
        to_partner(source, 0, me).wait_send()
        to_partner(source, 1, across).wait_send()
        part_to_partner(source, 0).wait_send()
        part_to_partner(source, 1).wait_send()
        pair_to_across(source).wait_send()

        @pl.when(source != here)
        def _():
            dispatch(source, here).wait_send()
            give_back(source, here).wait_send()
        return carry

    lax.fori_loop(0, sp_count, drain, 0)


def layer(
    sp_count, tp_count, cap, residual, q, k, v, gate, decay_in, offset, spikes, documents, weight,
    gains, shifts, routes, chosen, w_gate, w_up, w_down,
):
    rows, heads = spikes.shape
    tokens, width = residual.shape
    channels = q.shape[1]
    units = w_gate.shape[2]
    slots = sp_count * cap
    state_rows = v.shape[1] // heads + 16
    bf16, f32 = jnp.bfloat16, jnp.float32
    dma = pltpu.SemaphoreType.DMA
    inputs = (
        residual, q, k, v, gate, decay_in, offset.reshape(1, -1), spikes.T,
        documents.reshape(1, -1), routes.T, chosen.T, weight, gains, shifts, w_gate, w_up, w_down,
    )
    return pl.pallas_call(
        functools.partial(layer_kernel, heads, sp_count, tp_count, cap),
        out_shape=jax.ShapeDtypeStruct((tokens, width), bf16),
        in_specs=[pl.BlockSpec(memory_space=pltpu.HBM)] * len(inputs),
        out_specs=VMEM,
        scratch_shapes=[pltpu.VMEM(value.shape, value.dtype) for value in inputs[:14]]
        + [
            pltpu.VMEM((state_rows, channels), bf16),
            pltpu.VMEM((sp_count, state_rows, channels), bf16),
            pltpu.VMEM((state_rows - 16, channels), f32),
            pltpu.VMEM((1, channels), f32),
            pltpu.VMEM((1, channels), f32),
            pltpu.VMEM((rows, v.shape[1]), bf16),
            pltpu.VMEM((2, tokens, width), bf16),
            pltpu.VMEM((2, tokens, width), bf16),
            pltpu.VMEM((tokens, width), bf16),
            pltpu.VMEM((tokens, width), bf16),
            pltpu.VMEM((rows, channels), f32),
            pltpu.VMEM((tokens, width), bf16),
            pltpu.VMEM((slots, width), bf16),
            pltpu.VMEM((slots * tp_count, width), bf16),
            pltpu.VMEM((slots * tp_count, width), bf16),
            pltpu.VMEM((units // 128, width, 256), bf16),
            pltpu.VMEM((units, width), bf16),
            pltpu.VMEM((2 * tp_count * cap, units), bf16),
            pltpu.VMEM((slots * 2, width), bf16),
            pltpu.VMEM((slots, width), bf16),
            pltpu.VMEM((slots, width), bf16),
            pltpu.VMEM((slots, width), bf16),
            pltpu.VMEM((slots, width), bf16),
            dma((14,)),
            dma((sp_count,)),
            dma((sp_count,)),
            dma((2,)),
            dma((2,)),
            dma((2,)),
            dma((2 * (units // 128) + 1,)),
            dma((sp_count,)),
            dma((sp_count,)),
            dma((sp_count,)),
            dma((sp_count,)),
            dma((sp_count, 2)),
            dma((sp_count, 2)),
            dma((sp_count, 2)),
            dma((sp_count, 2)),
            dma((sp_count,)),
            dma((sp_count,)),
            dma((sp_count,)),
            dma((sp_count,)),
        ],
        compiler_params=pltpu.CompilerParams(
            collective_id=1, has_side_effects=True, vmem_limit_bytes=67043328
        ),
        name="layer",
    )(*inputs)


def slot_index(route_rows, block_rows, capacity, expert_count):
    row_total, top_count = route_rows.shape
    sources = row_total // block_rows
    flat_routes = route_rows.reshape(sources, block_rows * top_count)
    expert_marks = (
        flat_routes[:, :, None] == lax.broadcasted_iota(jnp.int32, (1, 1, expert_count), 2)
    ).astype(jnp.int32)
    before = jnp.cumsum(expert_marks, axis=1) - expert_marks
    position = jnp.sum(before * expert_marks, axis=2)
    source_id = lax.broadcasted_iota(jnp.int32, position.shape, 0)
    slots = flat_routes * (sources * capacity) + source_id * capacity + position
    return slots.reshape(row_total, top_count)


def fill_slots(row_block, slots, slot_total):
    owners = lax.broadcasted_iota(jnp.int32, slots.shape, 0).reshape(-1)
    slot_owner = (
        jnp.full((slot_total,), slots.shape[0], jnp.int32).at[slots.reshape(-1)].set(owners)
    )
    return jnp.take(row_block, slot_owner, axis=0, mode="fill", fill_value=0)


def expert_quarter(row_block, gate_part, up_part, down_part):
    gate_val = jnp.dot(row_block, gate_part, preferred_element_type=jnp.float32)
    up_val = jnp.dot(row_block, up_part, preferred_element_type=jnp.float32)
    hidden = (jax.nn.silu(gate_val) * up_val).astype(jnp.bfloat16)
    return jnp.dot(hidden, down_part, preferred_element_type=jnp.float32).astype(jnp.bfloat16)


def combine_rows(returned, slots, weight_rows):
    model_width = returned.shape[-1]
    picked = jnp.take(returned.reshape(-1, model_width), slots.reshape(-1), axis=0)
    picked = picked.reshape(slots.shape + (model_width,))
    return jnp.sum(picked * weight_rows[:, :, None], axis=1)


def on_device(
    residual,
    queries,
    projected_keys,
    values,
    projected_output_gate,
    decay_gate_input,
    decay_gate_offset,
    decay_spikes,
    documents,
    attention_output_weight,
    layer_norm_gains,
    layer_norm_shifts,
    routes,
    chosen_expert_weights,
    expert_gate_weight,
    expert_up_weight,
    expert_down_weight,
):
    sequence_length, head_number = decay_spikes.shape
    rows_dev, model_width = residual.shape
    expert_count = lax.axis_size("sp")
    capacity = max(2, 4 * rows_dev // expert_count)
    peers, parts = lax.axis_size("sp"), lax.axis_size("tp")
    channels = queries.shape[1]
    if (
        capacity % 16 == 0 and peers == 8 and parts == 4 and channels == 128
        and sequence_length % 128 == 0
    ):
        return layer(
            peers, parts, capacity, residual, queries, projected_keys, values,
            projected_output_gate, decay_gate_input, decay_gate_offset, decay_spikes, documents,
            attention_output_weight, layer_norm_gains, layer_norm_shifts, routes,
            chosen_expert_weights, expert_gate_weight, expert_up_weight, expert_down_weight,
        )
    normed = attention(
        peers, parts, residual, queries, projected_keys, values,
        projected_output_gate, decay_gate_input, decay_gate_offset, decay_spikes, documents,
        attention_output_weight, layer_norm_gains, layer_norm_shifts,
    )
    own_routes = lax.dynamic_slice_in_dim(routes, lax.axis_index("tp") * rows_dev, rows_dev, 0)
    own_weights = lax.dynamic_slice_in_dim(
        chosen_expert_weights, lax.axis_index("tp") * rows_dev, rows_dev, 0
    )
    slots = slot_index(own_routes, rows_dev, capacity, expert_count)
    outgoing = fill_slots(normed, slots, expert_count * capacity).reshape(
        expert_count, capacity, model_width
    )
    all_rows = lax.all_gather(
        lax.all_to_all(outgoing, "sp", split_axis=0, concat_axis=0, tiled=True),
        "tp",
        axis=1,
        tiled=True,
    )
    sources, slot_count, _ = all_rows.shape
    partial_value = expert_quarter(
        all_rows.reshape(sources * slot_count, model_width),
        expert_gate_weight[0],
        expert_up_weight[0],
        expert_down_weight[0],
    )
    summed = lax.psum_scatter(
        partial_value.reshape(sources, slot_count, model_width)
        .astype(jnp.float32)
        .astype(jnp.bfloat16),
        "tp",
        scatter_dimension=1,
        tiled=True,
    ).astype(jnp.float32)
    returned = lax.all_to_all(
        summed.astype(jnp.bfloat16), "sp", split_axis=0, concat_axis=0, tiled=True
    ).astype(summed.dtype)
    expert_mix = combine_rows(returned, slots, own_weights)
    return norm_rows(
        normed.astype(jnp.float32) + expert_mix, layer_norm_gains[1], layer_norm_shifts[1]
    ).astype(jnp.bfloat16)


def solution(mesh):
    placed = (
        P(("sp", "tp"), None),
        P("sp", "tp"),
        P("sp", "tp"),
        P("sp", "tp"),
        P("sp", "tp"),
        P("sp", "tp"),
        P("tp"),
        P("sp", "tp"),
        P("sp"),
        P("tp", None),
        P(),
        P(),
        P("sp", None),
        P("sp", None),
        P("sp", None, "tp"),
        P("sp", None, "tp"),
        P("sp", "tp", None),
    )
    return jax.shard_map(
        on_device, mesh=mesh, in_specs=placed, out_specs=P(("sp", "tp"), None), check_vma=False
    )
```
